32 devices in a mesh: sp: 8 (over z, x), tp: 4 (over y, core).
Axes of the slice: x: 2, y: 2, z: 4, core: 2. Of those that a mesh axis runs over, the one named last changes fastest.
Arguments:
- residual: bfloat16 [2560, 2048], P(('sp', 'tp')), may hold values from -6 to 6
- query_narrow: bfloat16 [2560, 1024], P('sp', 'tp'), may hold values from -48 to 48
- key_narrow: bfloat16 [2560, 1024], P('sp', 'tp'), may hold values from -48 to 48
- value_narrow: bfloat16 [2560, 1024], P('sp', 'tp'), may hold values from -6 to 6
- query_wide: bfloat16 [2560, 2048], P('sp', 'tp'), may hold values from -48 to 48
- key_wide: bfloat16 [2560, 2048], P('sp', 'tp'), may hold values from -48 to 48
- value_wide: bfloat16 [2560, 1024], P('sp', 'tp'), may hold values from -6 to 6
- subtract_narrow: float32 [8], P('tp'), may hold values from 0.3 to 0.8
- subtract_wide: float32 [8], P('tp'), may hold values from 0.3 to 0.8
- head_gain: float32 [128], replicated, may hold values from 0.1 to 1.9
- out_narrow: bfloat16 [1024, 2048], replicated, may hold values from -0.125 to 0.125
- out_wide: bfloat16 [1024, 2048], replicated, may hold values from -0.125 to 0.125
- norm1_gain: float32 [2048], replicated, may hold values from 0.1 to 1.9
- norm2_gain: float32 [2048], replicated, may hold values from 0.1 to 1.9
- expert_ids: int32 [2560, 2], P(('sp', 'tp')), may hold values from 0 to 7, all different within a row; in each aligned block of 80 rows (0 to 79, 80 to 159, ...) at most 30 rows name the same one
- expert_weight: float32 [2560, 2], P(('sp', 'tp')), may hold values from 0.1 to 1
- gate_proj: bfloat16 [8, 2048, 2048], P('sp', None, 'tp'), may hold values from -0.125 to 0.125
- up_proj: bfloat16 [8, 2048, 2048], P('sp', None, 'tp'), may hold values from -0.125 to 0.125
- down_proj: bfloat16 [8, 2048, 2048], P('sp', 'tp'), may hold values from -0.125 to 0.125
Outputs:
- layer_out: bfloat16 [2560, 2048], P(('sp', 'tp'))
The draws below stay inside these ranges and needn't reach their ends.
Inputs may be any that keep to these rules, and one draw needn't show every extreme that they name: `expert_ids`: each row names 2 different experts. Among the 80 rows of one device no expert is named more than 30 times, and in some device's rows some expert is named exactly 30 times.
All inputs are finite; a program needn't handle non-finite values.
Results may differ from the reference program's by a relative error of at most 0.014.
Values may be sent and summed in bfloat16 or wider, within the bound.
A program may use at most 128 MiB of HBM per device.

```python
import math
import jax
import jax.numpy as jnp
import numpy as np
from jax import lax

D = 2048
HG = 8
DKS = 64
DKB = 128
VD = 128
FF = 2048
TOPK = 2
TOK_DEV = 320
TOKENS = 2560
TR = 80
EXPERTS = 8
CAP = 30
N_TP = 4


def drawn_pair(key, key_size):
    width = HG * 2 * key_size
    key_query, key_keys = jax.random.split(key, 2)
    query = jnp.clip(1.3 * jax.random.normal(key_query, (TOKENS, width), jnp.float32), -5.2, 5.2)
    keys = jnp.clip(1.3 * jax.random.normal(key_keys, (TOKENS, width), jnp.float32), -5.2, 5.2)
    return (query, keys)


def draw_query_narrow(key, part):
    return drawn_pair(jax.random.fold_in(key, 11), DKS)[0].astype(jnp.bfloat16)


def draw_key_narrow(key, part):
    return drawn_pair(jax.random.fold_in(key, 11), DKS)[1].astype(jnp.bfloat16)


def draw_query_wide(key, part):
    return drawn_pair(jax.random.fold_in(key, 12), DKB)[0].astype(jnp.bfloat16)


def draw_key_wide(key, part):
    return drawn_pair(jax.random.fold_in(key, 12), DKB)[1].astype(jnp.bfloat16)


def shard_levels(key, dims, cuts, least, largest):
    def one(dim, parts):
        draws = jax.random.uniform(jax.random.fold_in(jax.random.fold_in(key, 6), dim), (parts,), jnp.float32, least / len(cuts), largest / len(cuts))
        return jnp.repeat(jnp.exp(draws), dims[dim] // parts).reshape((-1,) + (1,) * (len(dims) - dim - 1))

    loudness = one(*cuts[0])
    for cut in cuts[1:]:
        loudness = loudness * one(*cut)
    return loudness


def routed_block(stream_key, own, number, rows, amount, top, limit, slope):
    order = jax.random.permutation(stream_key, amount)
    crowded, ordinary = portions_of(amount, rows * top, limit, slope, True), portions_of(amount, rows * top, limit, slope, False)
    places = jnp.arange(amount)

    def named(sizes, rotation):
        used = int((sizes > 0).sum())
        fixed = max(1, used // 4)
        passed = fixed + (places - fixed + rotation * (used - fixed)) % max(1, amount - fixed)
        return jnp.zeros((amount,), jnp.int32).at[order[jnp.where(places < fixed, places, passed)]].set(jnp.asarray(sizes, jnp.int32))

    sizes = jnp.where(number % 4 == 0, named(crowded, number // 4), named(ordinary, number - number // 4 - 1))
    mixed = jax.random.permutation(jax.random.fold_in(own, 3), amount)
    giver, sink = mixed[0:amount // 2 * 2:2], mixed[1:amount // 2 * 2:2]
    room = jnp.minimum(sizes[giver] - 1, limit - sizes[sink]) // 2
    room = jnp.where((giver == order[0]) | (sink == order[0]) | (sizes[sink] == 0), 0, jnp.maximum(room, 0))
    passed = jax.random.randint(jax.random.fold_in(own, 4), (amount // 2,), 0, 1 << 20) % (room + 1)
    sizes = sizes.at[giver].add(-passed).at[sink].add(passed)
    items = jnp.searchsorted(jnp.cumsum(sizes), jnp.arange(rows * top), side="right").astype(jnp.int32)
    grid = items.reshape(top, rows).T
    grid = grid[jax.random.permutation(jax.random.fold_in(own, 1), rows)]
    rotation = jax.random.randint(jax.random.fold_in(own, 2), (rows, 1), 0, top)
    return jnp.take_along_axis(grid, (jnp.arange(top)[None, :] + rotation) % top, axis=1)


def portions_of(number_of, total, reach, skew, full):
    portions = [(1 << 20) // math.isqrt(rank ** skew) + 1 for rank in range(1, number_of + 1)]
    largest = reach if full else min(reach, max(-(-total // number_of), total * portions[0] // sum(portions)))
    least = 1 if total - largest >= number_of - 1 else 0
    given, rest = [largest] + [least] * (number_of - 1), total - largest - least * (number_of - 1)
    while rest > 0:
        candidates = [i for i in range(1, number_of) if given[i] < largest] or [i for i in range(1, number_of) if given[i] < reach]
        whole, left = sum([portions[i] for i in candidates]), rest
        for i in candidates:
            more = min(reach - given[i], max(1, left * portions[i] // whole), rest)
            given[i] = given[i] + more
            rest = rest - more
    return np.array(given)


def gaussian(rng, extent, scale, bound, shards=(), kind=jnp.bfloat16):
    result = scale * jax.random.normal(rng, extent, jnp.float32)
    if shards:
        result = result * shard_levels(rng, extent, shards, -0.22, 0.18)
    return jnp.clip(result, -bound, bound).astype(kind)


def setup_inputs(seed: int = 0) -> dict:
    seeds = jax.random.split(jax.random.key(seed), 20)
    residual = gaussian(seeds[0], (TOKENS, D), 1.0, 6.0, ((0, 32),))
    query_narrow = draw_query_narrow(jax.random.fold_in(seeds[19], 71), 0)
    key_narrow = draw_key_narrow(jax.random.fold_in(seeds[19], 71), 0)
    value_narrow = gaussian(seeds[3], (TOKENS, HG * VD), 1.0, 6.0, ((0, 8), (1, 4)))
    query_wide = draw_query_wide(jax.random.fold_in(seeds[19], 71), 0)
    key_wide = draw_key_wide(jax.random.fold_in(seeds[19], 71), 0)
    value_wide = gaussian(seeds[6], (TOKENS, HG * VD), 1.0, 6.0, ((0, 8), (1, 4)))
    subtract_narrow = jnp.clip(0.3 + 0.5 * jax.random.uniform(seeds[7], (HG,), jnp.float32) ** shard_levels(seeds[7], (HG,), ((0, 4),), -0.2, 0.2), 0.3, 0.8)
    subtract_wide = jnp.clip(0.3 + 0.5 * jax.random.uniform(seeds[8], (HG,), jnp.float32) ** shard_levels(seeds[8], (HG,), ((0, 4),), -0.2, 0.2), 0.3, 0.8)
    head_gain = jnp.clip(1.0 + 0.18 * jax.random.normal(seeds[9], (VD,), jnp.float32), 0.1, 1.9)
    out_narrow = gaussian(seeds[10], (HG * VD, D), (2 * HG * VD) ** -0.5, 0.125)
    out_wide = gaussian(seeds[11], (HG * VD, D), (2 * HG * VD) ** -0.5, 0.125)
    norm1_gain = jnp.clip(1.0 + 0.18 * jax.random.normal(seeds[12], (D,), jnp.float32), 0.1, 1.9)
    norm2_gain = jnp.clip(1.0 + 0.18 * jax.random.normal(seeds[13], (D,), jnp.float32), 0.1, 1.9)
    expert_ids_keys = jax.random.split(jax.random.fold_in(seeds[14], 1), TOKENS // TR)
    expert_ids_turns = jax.random.permutation(jax.random.fold_in(seeds[14], 3), TOKENS // TR)
    expert_ids = jax.vmap(lambda own, number: routed_block(jax.random.fold_in(seeds[14], 2), own, number, TR, EXPERTS, TOPK, CAP, 2))(expert_ids_keys, expert_ids_turns).reshape((TOKENS, TOPK))
    expert_weight = jnp.clip(0.1 + 0.9 * jax.random.uniform(seeds[15], (TOKENS, TOPK), jnp.float32) ** shard_levels(seeds[15], (TOKENS, TOPK), ((0, 32),), -0.2, 0.2), 0.1, 1.0)
    gate_proj = gaussian(seeds[16], (EXPERTS, D, FF), D ** -0.5, 0.125, ((0, 8), (2, 4)))
    up_proj = gaussian(seeds[17], (EXPERTS, D, FF), D ** -0.5, 0.125, ((0, 8), (2, 4)))
    down_proj = gaussian(seeds[18], (EXPERTS, FF, D), FF ** -0.5, 0.125, ((0, 8), (1, 4)))
    return {"residual": residual, "query_narrow": query_narrow, "key_narrow": key_narrow, "value_narrow": value_narrow, "query_wide": query_wide, "key_wide": key_wide, "value_wide": value_wide, "subtract_narrow": subtract_narrow, "subtract_wide": subtract_wide, "head_gain": head_gain, "out_narrow": out_narrow, "out_wide": out_wide, "norm1_gain": norm1_gain, "norm2_gain": norm2_gain, "expert_ids": expert_ids, "expert_weight": expert_weight, "gate_proj": gate_proj, "up_proj": up_proj, "down_proj": down_proj}


residual_scale = 2.0 ** 0.5

def layer_norm(values, gain):
    center = lax.optimization_barrier(jnp.mean(values, -1, keepdims=True))
    spread = lax.optimization_barrier(jnp.mean(jnp.square(values - center), -1, keepdims=True))
    return (values - center) * lax.rsqrt(spread + 1e-05) * gain

def attend_block(block, keys, values, subtract, head_gain, key_size):
    scores = jnp.einsum('qhmd,khmd->hmqk', block.astype(jnp.float32), keys.astype(jnp.float32)) * key_size ** (-0.5)
    rowtop = lax.optimization_barrier(jnp.max(scores, -1, keepdims=True))
    expo = jnp.exp(scores - rowtop)
    total = lax.optimization_barrier(jnp.sum(expo, -1))
    weights = expo.astype(jnp.bfloat16)
    mapped = jnp.einsum('hmqk,khe->hmqe', weights.astype(jnp.float32), values.astype(jnp.float32)) / total[..., None]
    diff = mapped[:, 0] - subtract[:, None, None] * mapped[:, 1]
    normed = diff * lax.rsqrt(lax.optimization_barrier(jnp.mean(diff * diff, -1, keepdims=True)) + 1e-06) * head_gain
    return jnp.transpose(normed, (1, 0, 2)).reshape(block.shape[0], -1).astype(jnp.bfloat16)

def attend(query, keys, values, subtract, head_gain):
    tokens = query.shape[0]
    head_count = subtract.shape[0]
    key_size = query.shape[1] // (2 * head_count)
    queries = query.reshape(tokens, head_count, 2, key_size)
    key_rows = keys.reshape(tokens, head_count, 2, key_size)
    value_rows = values.reshape(tokens, head_count, -1)
    span = math.gcd(tokens, 256)
    blocks = queries.reshape(tokens // span, span, head_count, 2, key_size)

    def one_block(block):
        return attend_block(block, key_rows, value_rows, subtract, head_gain, key_size)
    return lax.map(one_block, blocks).reshape(tokens, -1)

def experts_output(hidden, expert_ids, expert_weight, gate_proj, up_proj, down_proj):
    tokens, top_count = expert_ids.shape
    experts = gate_proj.shape[0]
    rows = TOK_DEV // N_TP
    blocks = tokens // rows
    capacity = max(2, 3 * rows * top_count // (2 * experts))
    ids = expert_ids.reshape(blocks, rows * top_count)
    onehot = (ids[..., None] == jnp.arange(experts, dtype=jnp.int32)).astype(jnp.int32)
    before = jnp.cumsum(onehot, 1) - onehot
    position = lax.optimization_barrier(jnp.sum(before * onehot, -1)).astype(jnp.int32)
    column = jnp.arange(blocks, dtype=jnp.int32)[:, None] * capacity + position
    owner = jnp.repeat(jnp.arange(tokens, dtype=jnp.int32), top_count).reshape(blocks, rows * top_count)
    table = jnp.full((experts, blocks * capacity), tokens, jnp.int32)
    table = table.at[ids.reshape(-1), column.reshape(-1)].set(owner.reshape(-1))
    padded = jnp.concatenate([hidden, jnp.zeros((1, hidden.shape[1]), jnp.bfloat16)], 0)
    width = gate_proj.shape[2] // N_TP

    def one_expert(operands):
        picks, w_gate, w_up, w_down = operands
        taken = padded[picks]
        summed = jnp.zeros((picks.shape[0], hidden.shape[1]), jnp.float32)
        for piece in range(N_TP):
            gate_part = jnp.dot(taken, w_gate[:, piece * width:(piece + 1) * width], preferred_element_type=jnp.float32)
            up_part = jnp.dot(taken, w_up[:, piece * width:(piece + 1) * width], preferred_element_type=jnp.float32)
            inner = (jax.nn.silu(gate_part) * up_part).astype(jnp.bfloat16)
            partial_out = jnp.dot(inner, w_down[piece * width:(piece + 1) * width], preferred_element_type=jnp.float32)
            rounded = lax.optimization_barrier(partial_out.astype(jnp.bfloat16))
            summed = summed + rounded.astype(jnp.float32)
        return summed.astype(jnp.bfloat16)
    results = lax.map(one_expert, (table, gate_proj, up_proj, down_proj))
    flat = results.reshape(experts * blocks * capacity, -1)
    where_rows = (ids * (blocks * capacity) + column).reshape(tokens, top_count)
    gathered = flat[where_rows].astype(jnp.float32)
    return lax.optimization_barrier(jnp.sum(expert_weight[..., None] * gathered, 1))

def reference(residual, query_narrow, key_narrow, value_narrow, query_wide, key_wide, value_wide, subtract_narrow, subtract_wide, head_gain, out_narrow, out_wide, norm1_gain, norm2_gain, expert_ids, expert_weight, gate_proj, up_proj, down_proj):
    attended_narrow = attend(query_narrow, key_narrow, value_narrow, subtract_narrow, head_gain)
    attended_wide = attend(query_wide, key_wide, value_wide, subtract_wide, head_gain)
    mix = jnp.dot(attended_narrow, out_narrow, preferred_element_type=jnp.float32) + jnp.dot(attended_wide, out_wide, preferred_element_type=jnp.float32)
    hidden = layer_norm(residual_scale * residual.astype(jnp.float32) + mix, norm1_gain).astype(jnp.bfloat16)
    routed = experts_output(hidden, expert_ids, expert_weight, gate_proj, up_proj, down_proj)
    return layer_norm(residual_scale * hidden.astype(jnp.float32) + routed, norm2_gain).astype(jnp.bfloat16)
```

```python
import functools
import math

import jax
import jax.numpy as jnp
from jax import lax
from jax.experimental import pallas as pl
from jax.experimental.pallas import tpu as pltpu
from jax.sharding import PartitionSpec as P

residual_scale = 2.0**0.5


def layer_norm(values, gain):
    center = jnp.mean(values, -1, keepdims=True)
    spread = jnp.mean(jnp.square(values - center), -1, keepdims=True)
    return (values - center) * lax.rsqrt(spread + 1e-05) * gain


def block_take(shards, shard_rows):
    take = shards
    for count in range(shards, 0, -1):
        if shards % count == 0 and count * shard_rows >= 512:
            take = count
    return take


def start_carry(head_count, tok_rows, value_size):
    return (
        jnp.full((head_count, 2, tok_rows), -1e30, jnp.float32),
        jnp.zeros((head_count, 2, tok_rows), jnp.float32),
        jnp.zeros((head_count, 2, tok_rows, value_size), jnp.float32),
    )


def absorb_keys(carry, queries, key_piece, value_piece, shard_rows):
    head_count = queries.shape[1]
    key_size = queries.shape[3]
    shards = key_piece.shape[0] // shard_rows
    take = block_take(shards, shard_rows)
    span = take * shard_rows

    def one_block(step_index, state):
        rowtop, total, summed = state
        key_block = lax.dynamic_slice_in_dim(key_piece, step_index * span, span, 0).reshape(
            span, head_count, 2, key_size
        )
        value_block = lax.dynamic_slice_in_dim(value_piece, step_index * span, span, 0).reshape(
            span, head_count, -1
        )
        scores = jnp.einsum(
            "qhmd,khmd->hmqk", queries, key_block, preferred_element_type=jnp.float32
        ) * key_size ** (-0.5)
        newtop = jnp.maximum(rowtop, jnp.max(scores, -1))
        shrink = jnp.exp(rowtop - newtop)
        expo = jnp.exp(scores - newtop[..., None])
        total = total * shrink + jnp.sum(expo, -1)
        summed = summed * shrink[..., None] + jnp.einsum(
            "hmqk,khe->hmqe",
            expo.astype(jnp.bfloat16),
            value_block,
            preferred_element_type=jnp.float32,
        )
        return (newtop, total, summed)

    return lax.fori_loop(0, shards // take, one_block, carry)


def finish_heads(carry, subtract, head_gain):
    rowtop, total, summed = carry
    mapped = summed / total[..., None]
    diff = mapped[:, 0] - subtract[:, None, None] * mapped[:, 1]
    normed = diff * lax.rsqrt(jnp.mean(diff * diff, -1, keepdims=True) + 1e-06) * head_gain
    return jnp.transpose(normed, (1, 0, 2)).reshape(diff.shape[1], -1).astype(jnp.bfloat16)


def attend_kernel(
    narrow_sub_ref,
    wide_sub_ref,
    gain_ref,
    query_narrow_ref,
    key_narrow_ref,
    value_narrow_ref,
    query_wide_ref,
    key_wide_ref,
    value_wide_ref,
    out_ref,
    query_all,
    key_all,
    value_all,
    own,
    landed,
    send_sem,
    recv_sem,
    pass_send,
    pass_recv,
    out_send,
    out_recv,
):
    ranks = lax.axis_size("tp")
    me, rank = lax.axis_index("sp"), lax.axis_index("tp")
    layer, side = me // 2, lax.rem(me, 2)
    partner = me + 1 - 2 * side
    tok_rows = key_narrow_ref.shape[0]
    head_count = narrow_sub_ref.shape[0]
    layers = 2 * head_count
    out_rows, lanes = landed.shape[0], gain_ref.shape[1]
    narrow_size = lanes // 2

    def is_wide(index):
        return lax.rem((index + 1) // 2, 2) if not isinstance(index, int) else (index + 1) // 2 % 2

    wide, my_head = is_wide(layer), layer // 2

    def visit(step):
        return (
            layer,
            layer + 1 - 2 * lax.rem(layer, 2),
            lax.rem(layer + 2, layers),
            layers - 1 - layer,
        )[step]

    def piece(kind, target):
        head = target // 2
        value = pl.ds(head * lanes, lanes)
        if not is_wide(target):
            return (key_narrow_ref, None, value_narrow_ref, query_narrow_ref, None)[kind].at[:, value]
        if kind == 2:
            return value_wide_ref.at[:, value]
        ref = key_wide_ref if kind < 2 else query_wide_ref
        return ref.at[:, pl.ds((2 * head + kind % 3) * lanes, lanes)]

    def place(kind, index, half):
        row = 2 * index + half if kind < 3 else index
        at = pl.ds(pl.multiple_of(row * tok_rows, tok_rows), tok_rows)
        if kind == 2:
            return value_all.at[at, pl.ds(0, lanes)]
        return key_all.at[kind, at, :] if kind < 2 else query_all.at[kind - 3, at, :]

    def when_mine(kind, action):
        if kind in (1, 4):
            pl.when(wide == 1)(action)
        else:
            action()

    def to_layer(kind, target):
        return pltpu.make_async_remote_copy(
            src_ref=piece(kind, target),
            dst_ref=place(kind, layer, side),
            send_sem=send_sem.at[kind, target],
            recv_sem=recv_sem.at[kind, layer],
            device_id={"sp": 2 * target + side},
            device_id_type=pl.DeviceIdType.MESH,
        )

    def kinds_for(target, kinds):
        return [kind for kind in kinds if is_wide(target) or kind not in (1, 4)]

    for kinds in ((0, 1, 2), (3, 4)):
        for target in sorted(range(layers), key=lambda index: -is_wide(index)):
            for kind in kinds_for(target, kinds):

                @pl.when(layer != target)
                def _():
                    to_layer(kind, target).start()

                @pl.when(layer == target)
                def _():
                    pltpu.make_async_copy(
                        piece(kind, target), place(kind, target, side), recv_sem.at[kind, target]
                    ).start()

    value_all[:, lanes:] = jnp.ones((value_all.shape[0], lanes), jnp.bfloat16)

    def landed_here(kind, index, half, sem):
        where = place(kind, index, half)
        pltpu.make_async_copy(where, where, sem.at[kind, index]).wait()

    def pass_on(kind, index):
        where = place(kind, index, side)
        return pltpu.make_async_remote_copy(
            src_ref=where,
            dst_ref=where,
            send_sem=pass_send.at[kind, index],
            recv_sem=pass_recv.at[kind, index],
            device_id={"sp": partner},
            device_id_type=pl.DeviceIdType.MESH,
        )

    for step in range(layers):
        index = visit(step)
        for kind in range(3):

            def forward():
                landed_here(kind, index, side, recv_sem)
                pass_on(kind, index).start()

            when_mine(kind, forward)
    for step in range(layers):
        index = visit(step)
        for kind in range(3):
            when_mine(kind, lambda: landed_here(kind, index, 1 - side, pass_recv))

    scale = math.log2(math.e) * jnp.where(wide == 1, lanes ** (-0.5), narrow_size ** (-0.5))
    scale = scale.astype(jnp.float32)
    subtract = jnp.where(wide == 1, wide_sub_ref[my_head], narrow_sub_ref[my_head])
    column = wide * (head_count * ranks) + rank * head_count + my_head

    def to_tokens(index, part):
        row = pl.multiple_of(index * tok_rows + part * out_rows, out_rows)
        source = own.at[pl.ds(row, out_rows), :]
        there = landed.at[:, pl.ds(pl.multiple_of(column * lanes, lanes), lanes)]
        block = 2 * index + side
        remote = pltpu.make_async_remote_copy(
            src_ref=source,
            dst_ref=there,
            send_sem=out_send.at[index, part],
            recv_sem=out_recv.at[column],
            device_id={"sp": block, "tp": part},
            device_id_type=pl.DeviceIdType.MESH,
        )
        here = pltpu.make_async_copy(source, there, out_recv.at[column])
        return remote, here, (block == me) & (rank == part)

    lane = lax.broadcasted_iota(jnp.int32, (tok_rows, lanes), 1)
    for step in range(layers):
        index = visit(step)
        for kind in (3, 4):
            when_mine(kind, lambda: landed_here(kind, index, side, recv_sem))
        at = pl.ds(pl.multiple_of(index * tok_rows, tok_rows), tok_rows)
        mapped = []
        for part in range(2):
            low = jnp.where(wide == 1, 0, part * narrow_size)
            high = jnp.where(wide == 1, lanes, (part + 1) * narrow_size)
            plane = part * wide
            queries = jnp.where(
                (lane >= low) & (lane < high), query_all[plane, at, :].astype(jnp.float32), 0.0
            ).astype(jnp.bfloat16)
            scores = lax.dot_general(
                queries,
                key_all[plane],
                (((1,), (1,)), ((), ())),
                preferred_element_type=jnp.float32,
            )
            top = jnp.max(scores, -1, keepdims=True)
            expo = jnp.exp2(scores * scale - top * scale).astype(jnp.bfloat16)
            summed = jnp.dot(expo, value_all[...], preferred_element_type=jnp.float32)
            mapped.append(summed[:, :lanes] / summed[:, lanes:])
        diff = mapped[0] - subtract * mapped[1]
        normed = diff * lax.rsqrt(jnp.mean(diff * diff, -1, keepdims=True) + 1e-06) * gain_ref[...]
        own[at, :] = normed.astype(jnp.bfloat16)
        for part in range(ranks):
            remote, here, mine = to_tokens(index, part)

            @pl.when(mine)
            def _():
                here.start()

            @pl.when(jnp.logical_not(mine))
            def _():
                remote.start()

    for target in range(layers):
        for kind in kinds_for(target, range(5)):

            @pl.when(layer != target)
            def _():
                to_layer(kind, target).wait_send()

    for index in range(layers):
        for kind in range(3):
            when_mine(kind, lambda: pass_on(kind, index).wait_send())
        for part in range(ranks):
            remote, here, mine = to_tokens(index, part)

            @pl.when(jnp.logical_not(mine))
            def _():
                remote.wait_send()

    for head in range(layers * ranks):
        where = landed.at[:, pl.ds(head * lanes, lanes)]
        pltpu.make_async_copy(where, where, out_recv.at[head]).wait()
    out_ref[...] = landed[...]


def attend_by_head(queries, keys, values, subtract_narrow, subtract_wide, head_gain, out_rows):
    shards, ranks = lax.axis_size("sp"), lax.axis_size("tp")
    head_count, lanes = subtract_narrow.shape[0], head_gain.shape[0]
    tok_rows = keys[0].shape[0]
    tokens, layers = shards * tok_rows, 2 * head_count
    heads = layers * ranks
    vmem = pl.BlockSpec(memory_space=pltpu.VMEM)
    smem = pl.BlockSpec(memory_space=pltpu.SMEM)
    dma = pltpu.SemaphoreType.DMA
    return pl.pallas_call(
        attend_kernel,
        out_shape=jax.ShapeDtypeStruct((out_rows, heads * lanes), jnp.bfloat16),
        in_specs=[smem, smem, vmem] + [pl.BlockSpec(memory_space=pl.ANY)] * 6,
        out_specs=vmem,
        scratch_shapes=[
            pltpu.VMEM((2, layers * tok_rows, lanes), jnp.bfloat16),
            pltpu.VMEM((2, tokens, lanes), jnp.bfloat16),
            pltpu.VMEM((tokens, 2 * lanes), jnp.bfloat16),
            pltpu.VMEM((layers * tok_rows, lanes), jnp.bfloat16),
            pltpu.VMEM((out_rows, heads * lanes), jnp.bfloat16),
            dma((5, layers)),
            dma((5, layers)),
            dma((3, layers)),
            dma((3, layers)),
            dma((layers, ranks)),
            dma((heads,)),
        ],
        compiler_params=pltpu.CompilerParams(
            has_side_effects=True, vmem_limit_bytes=40 * 1024 * 1024
        ),
    )(
        subtract_narrow,
        subtract_wide,
        head_gain[None],
        queries[0],
        keys[0],
        values[0],
        queries[1],
        keys[1],
        values[1],
    )


def head_split_fits(tok_rows, out_rows, ranks, heads, shards, value_size, key_sizes):
    return (
        heads == 2
        and shards == 4 * heads
        and out_rows * ranks == tok_rows
        and tok_rows % 16 == 0
        and out_rows % 16 == 0
        and value_size == 128
        and key_sizes == (value_size // 2, value_size)
    )


def expert_kernel(
    send_ref,
    gate_ref,
    up_ref,
    down_ref,
    out_ref,
    rows,
    part,
    pairs,
    mid,
    cross,
    done,
    back,
    far_send,
    far_recv,
    near_send,
    near_recv,
    sum_send,
    sum_recv,
    back_send,
    back_recv,
):
    shards, ranks = lax.axis_size("sp"), lax.axis_size("tp")
    me, rank = lax.axis_index("sp"), lax.axis_index("tp")
    cap = send_ref.shape[0] // shards
    side, core = rank // 2, lax.rem(rank, 2)
    partner, across = rank + 1 - 2 * core, lax.rem(rank + 2, ranks)
    my_place, far_place = core * 2 + side, core * 2 + 1 - side
    block = ranks * cap

    def at(ref, index, count=1):
        return ref.at[pl.ds(pl.multiple_of(index * cap, cap), count * cap), :]

    def copy_to(source, place, send, recv, device):
        return pltpu.make_async_remote_copy(
            src_ref=source,
            dst_ref=place,
            send_sem=send,
            recv_sem=recv,
            device_id=device,
            device_id_type=pl.DeviceIdType.MESH,
        )

    def far(hop):
        target = lax.rem(me + hop, shards)
        return copy_to(
            at(send_ref, target),
            at(rows, hop * ranks + my_place),
            far_send.at[hop],
            far_recv.at[hop],
            {"sp": target},
        )

    def near(kind, hop):
        place = far_place if kind == 2 else my_place
        piece = at(rows, hop * ranks + place)
        device = {"tp": across if kind == 1 else partner}
        return copy_to(piece, piece, near_send.at[kind, hop], near_recv.at[kind, hop], device)

    def pair_sum(hop):
        return copy_to(
            at(part, hop * ranks + (1 - core) * 2, 2),
            at(pairs, hop * 2, 2),
            sum_send.at[0, hop],
            sum_recv.at[0, hop],
            {"tp": partner},
        )

    def cross_sum(hop):
        return copy_to(
            at(mid, hop), at(cross, hop), sum_send.at[1, hop], sum_recv.at[1, hop], {"tp": across}
        )

    def give_back(hop):
        return copy_to(
            at(done, hop),
            at(back, me),
            back_send.at[hop],
            back_recv.at[hop],
            {"sp": lax.rem(me - hop + shards, shards)},
        )

    @pl.loop(1, shards)
    def _(hop):
        far(hop).start()

    own_rows = pltpu.make_async_copy(at(send_ref, me), at(rows, my_place), far_recv.at[0])
    own_rows.start()
    own_rows.wait()

    def share(hop):
        @pl.when(hop > 0)
        def _():
            far(hop).wait_recv()

        near(0, hop).start()
        near(1, hop).start()

    def relay(hop):
        near(1, hop).wait_recv()
        near(2, hop).start()

    def compute(hop):
        near(0, hop).wait_recv()
        near(2, hop).wait_recv()
        span = pl.ds(pl.multiple_of(hop * block, block), block)
        taken = rows[span, :]
        gate = jnp.dot(taken, gate_ref[...], preferred_element_type=jnp.float32)
        up = jnp.dot(taken, up_ref[...], preferred_element_type=jnp.float32)
        inner = (jax.nn.silu(gate) * up).astype(jnp.bfloat16)
        part[span, :] = jnp.dot(inner, down_ref[...], preferred_element_type=jnp.float32).astype(
            jnp.bfloat16
        )
        pair_sum(hop).start()

    def both(hop, place):
        mine = at(part, hop * ranks + core * 2 + place)[...].astype(jnp.float32)
        return mine + at(pairs, hop * 2 + place)[...].astype(jnp.float32)

    def add_pair(hop):
        pair_sum(hop).wait_recv()
        at(mid, hop)[...] = both(hop, 1 - side).astype(jnp.bfloat16)
        cross_sum(hop).start()

    def finish(hop):
        cross_sum(hop).wait_recv()
        total = both(hop, side) + at(cross, hop)[...].astype(jnp.float32)
        at(done, hop)[...] = total.astype(jnp.bfloat16)

        @pl.when(hop > 0)
        def _():
            give_back(hop).start()

    stages = (share, relay, compute, add_pair, finish)

    @pl.loop(0, shards + len(stages) - 1)
    def _(step):
        for late, stage in enumerate(stages):
            hop = step - late

            @pl.when((hop >= 0) & (hop < shards))
            def _():
                stage(hop)

    own_back = pltpu.make_async_copy(at(done, 0), at(back, me), back_recv.at[0])
    own_back.start()
    own_back.wait()

    @pl.loop(0, shards)
    def _(hop):
        for kind in range(3):
            near(kind, hop).wait_send()
        pair_sum(hop).wait_send()
        cross_sum(hop).wait_send()

        @pl.when(hop > 0)
        def _():
            far(hop).wait_send()
            give_back(hop).wait_send()
            copy_to(
                at(done, hop),
                at(back, lax.rem(me + hop, shards)),
                back_send.at[hop],
                back_recv.at[hop],
                {"sp": lax.rem(me + hop, shards)},
            ).wait_recv()

    out_ref[...] = back[...]


def experts_by_source(outgoing, gate, up, down):
    shards, ranks = lax.axis_size("sp"), lax.axis_size("tp")
    total, width = outgoing.shape
    vmem = pl.BlockSpec(memory_space=pltpu.VMEM)
    dma = pltpu.SemaphoreType.DMA
    return pl.pallas_call(
        expert_kernel,
        out_shape=jax.ShapeDtypeStruct((total, width), jnp.bfloat16),
        in_specs=[vmem] * 4,
        out_specs=vmem,
        scratch_shapes=[
            pltpu.VMEM((count * total, width), jnp.bfloat16)
            for count in (ranks, ranks, 2, 1, 1, 1, 1)
        ]
        + [
            dma((shards,)),
            dma((shards,)),
            dma((3, shards)),
            dma((3, shards)),
            dma((2, shards)),
            dma((2, shards)),
            dma((shards,)),
            dma((shards,)),
        ],
        compiler_params=pltpu.CompilerParams(
            has_side_effects=True, vmem_limit_bytes=56 * 1024 * 1024
        ),
    )(outgoing, gate, up, down)


def on_device(
    residual,
    query_narrow,
    key_narrow,
    value_narrow,
    query_wide,
    key_wide,
    value_wide,
    subtract_narrow,
    subtract_wide,
    head_gain,
    out_narrow,
    out_wide,
    norm1_gain,
    norm2_gain,
    expert_ids,
    expert_weight,
    gate_proj,
    up_proj,
    down_proj,
):
    tok_rows = query_narrow.shape[0]
    head_count = subtract_narrow.shape[0]
    value_size = head_gain.shape[0]
    if head_split_fits(
        tok_rows,
        residual.shape[0],
        lax.axis_size("tp"),
        head_count,
        lax.axis_size("sp"),
        value_size,
        tuple(part.shape[1] // (2 * head_count) for part in (key_narrow, key_wide)),
    ):
        attended = attend_by_head(
            (query_narrow, query_wide),
            (key_narrow, key_wide),
            (value_narrow, value_wide),
            subtract_narrow,
            subtract_wide,
            head_gain,
            residual.shape[0],
        )
        full_narrow, full_wide = jnp.split(attended, 2, 1)
    else:
        narrow_queries = query_narrow.reshape(tok_rows, head_count, 2, -1)
        wide_queries = query_wide.reshape(tok_rows, head_count, 2, -1)
        narrow_start = start_carry(head_count, tok_rows, value_size)
        wide_start = start_carry(head_count, tok_rows, value_size)
        narrow_state = absorb_keys(
            narrow_start,
            narrow_queries,
            lax.all_gather(key_narrow, "sp", axis=0, tiled=True),
            lax.all_gather(value_narrow, "sp", axis=0, tiled=True),
            tok_rows,
        )
        wide_state = absorb_keys(
            wide_start,
            wide_queries,
            lax.all_gather(key_wide, "sp", axis=0, tiled=True),
            lax.all_gather(value_wide, "sp", axis=0, tiled=True),
            tok_rows,
        )
        attended_narrow = finish_heads(narrow_state, subtract_narrow, head_gain)
        attended_wide = finish_heads(wide_state, subtract_wide, head_gain)
        full_narrow, full_wide = (
            lax.all_to_all(attended_narrow, "tp", split_axis=0, concat_axis=1, tiled=True),
            lax.all_to_all(attended_wide, "tp", split_axis=0, concat_axis=1, tiled=True),
        )
    mix = jnp.dot(full_narrow, out_narrow, preferred_element_type=jnp.float32) + jnp.dot(
        full_wide, out_wide, preferred_element_type=jnp.float32
    )
    hidden = layer_norm(residual_scale * residual.astype(jnp.float32) + mix, norm1_gain).astype(
        jnp.bfloat16
    )
    local_rows, top_count = expert_ids.shape
    experts = lax.axis_size("sp")
    capacity = max(2, 3 * local_rows * top_count // (2 * experts))
    in_kernel = lax.axis_size("tp") == 4 and 4 * experts * capacity * residual.shape[1] < 2**23
    if in_kernel:
        capacity = -(-capacity // 16) * 16
    flat_ids = expert_ids.reshape(-1)
    onehot = (flat_ids[:, None] == jnp.arange(experts, dtype=jnp.int32)[None, :]).astype(jnp.int32)
    before = jnp.cumsum(onehot, 0) - onehot
    position = jnp.sum(before * onehot, 1)
    slots = (flat_ids * capacity + position).reshape(local_rows, top_count)
    dispatch_table = jnp.any(
        jnp.arange(experts * capacity, dtype=jnp.int32)[:, None, None] == slots[None], -1
    ).astype(jnp.bfloat16)
    outgoing = jnp.dot(dispatch_table, hidden, preferred_element_type=jnp.float32).astype(
        jnp.bfloat16
    )
    if in_kernel:
        returned_flat = experts_by_source(outgoing, gate_proj[0], up_proj[0], down_proj[0])
        named = slots[..., None] == jnp.arange(experts * capacity, dtype=jnp.int32)
        combine = jnp.sum(jnp.where(named, expert_weight[..., None], 0.0), 1)
        routed = jnp.dot(
            combine, returned_flat.astype(jnp.float32), precision=lax.Precision.HIGHEST
        )
    else:
        outgoing = outgoing.reshape(experts, capacity, -1)
        gathered = lax.all_gather(
            lax.all_to_all(outgoing, "sp", split_axis=0, concat_axis=0, tiled=True),
            "tp",
            axis=1,
            tiled=True,
        )
        flat_rows = gathered.reshape(-1, gathered.shape[2])
        gate_part = jnp.dot(flat_rows, gate_proj[0], preferred_element_type=jnp.float32)
        up_part = jnp.dot(flat_rows, up_proj[0], preferred_element_type=jnp.float32)
        inner = (jax.nn.silu(gate_part) * up_part).astype(jnp.bfloat16)
        partial_out = jnp.dot(inner, down_proj[0], preferred_element_type=jnp.float32).reshape(
            gathered.shape
        )
        summed = lax.psum_scatter(
            partial_out.astype(jnp.bfloat16), "tp", scatter_dimension=1, tiled=True
        )
        returned = lax.all_to_all(summed, "sp", split_axis=0, concat_axis=0, tiled=True)
        returned_flat = returned.reshape(experts * capacity, -1)
        picked = returned_flat[slots].astype(jnp.float32)
        routed = jnp.sum(expert_weight[..., None] * picked, 1)
    return layer_norm(residual_scale * hidden.astype(jnp.float32) + routed, norm2_gain).astype(
        jnp.bfloat16
    )


def solution(mesh):
    placed = (
        P(("sp", "tp"), None),
        P("sp", "tp"),
        P("sp", "tp"),
        P("sp", "tp"),
        P("sp", "tp"),
        P("sp", "tp"),
        P("sp", "tp"),
        P("tp"),
        P("tp"),
        P(),
        P(),
        P(),
        P(),
        P(),
        P(("sp", "tp"), None),
        P(("sp", "tp"), None),
        P("sp", None, "tp"),
        P("sp", None, "tp"),
        P("sp", "tp", None),
    )
    return jax.shard_map(
        on_device, mesh=mesh, in_specs=placed, out_specs=P(("sp", "tp"), None), check_vma=False
    )
```

```python
import functools
import math

import jax
import jax.numpy as jnp
from jax import lax
from jax.experimental import pallas as pl
from jax.experimental.pallas import tpu as pltpu
from jax.sharding import PartitionSpec as P

residual_scale = 2.0**0.5


def layer_norm(values, gain):
    center = jnp.mean(values, -1, keepdims=True)
    spread = jnp.mean(jnp.square(values - center), -1, keepdims=True)
    return (values - center) * lax.rsqrt(spread + 1e-05) * gain


def block_take(shards, shard_rows):
    take = shards
    for count in range(shards, 0, -1):
        if shards % count == 0 and count * shard_rows >= 512:
            take = count
    return take


def start_carry(head_count, tok_rows, value_size):
    return (
        jnp.full((head_count, 2, tok_rows), -1e30, jnp.float32),
        jnp.zeros((head_count, 2, tok_rows), jnp.float32),
        jnp.zeros((head_count, 2, tok_rows, value_size), jnp.float32),
    )


def absorb_keys(carry, queries, key_piece, value_piece, shard_rows):
    head_count = queries.shape[1]
    key_size = queries.shape[3]
    shards = key_piece.shape[0] // shard_rows
    take = block_take(shards, shard_rows)
    span = take * shard_rows

    def one_block(step_index, state):
        rowtop, total, summed = state
        key_block = lax.dynamic_slice_in_dim(key_piece, step_index * span, span, 0).reshape(
            span, head_count, 2, key_size
        )
        value_block = lax.dynamic_slice_in_dim(value_piece, step_index * span, span, 0).reshape(
            span, head_count, -1
        )
        scores = jnp.einsum(
            "qhmd,khmd->hmqk", queries, key_block, preferred_element_type=jnp.float32
        ) * key_size ** (-0.5)
        newtop = jnp.maximum(rowtop, jnp.max(scores, -1))
        shrink = jnp.exp(rowtop - newtop)
        expo = jnp.exp(scores - newtop[..., None])
        total = total * shrink + jnp.sum(expo, -1)
        summed = summed * shrink[..., None] + jnp.einsum(
            "hmqk,khe->hmqe",
            expo.astype(jnp.bfloat16),
            value_block,
            preferred_element_type=jnp.float32,
        )
        return (newtop, total, summed)

    return lax.fori_loop(0, shards // take, one_block, carry)


def finish_heads(carry, subtract, head_gain):
    rowtop, total, summed = carry
    mapped = summed / total[..., None]
    diff = mapped[:, 0] - subtract[:, None, None] * mapped[:, 1]
    normed = diff * lax.rsqrt(jnp.mean(diff * diff, -1, keepdims=True) + 1e-06) * head_gain
    return jnp.transpose(normed, (1, 0, 2)).reshape(diff.shape[1], -1).astype(jnp.bfloat16)


def greet(peers):
    barrier = pltpu.get_barrier_semaphore()
    for peer in peers:
        pl.semaphore_signal(
            barrier, inc=1, device_id=peer, device_id_type=pl.DeviceIdType.MESH
        )
    pl.semaphore_wait(barrier, len(peers))


def attend_kernel(
    narrow_sub_ref,
    wide_sub_ref,
    gain_ref,
    query_narrow_ref,
    key_narrow_ref,
    value_narrow_ref,
    query_wide_ref,
    key_wide_ref,
    value_wide_ref,
    out_ref,
    query_all,
    key_all,
    value_all,
    own,
    landed,
    send_sem,
    recv_sem,
    pass_send,
    pass_recv,
    out_send,
    out_recv,
):
    ranks = lax.axis_size("tp")
    me, rank = lax.axis_index("sp"), lax.axis_index("tp")
    layer, side = me // 2, lax.rem(me, 2)
    partner = me + 1 - 2 * side
    tok_rows = key_narrow_ref.shape[0]
    head_count = narrow_sub_ref.shape[0]
    layers = 2 * head_count
    out_rows, lanes = landed.shape[0], gain_ref.shape[1]
    narrow_size = lanes // 2

    def is_wide(index):
        return lax.rem((index + 1) // 2, 2) if not isinstance(index, int) else (index + 1) // 2 % 2

    wide, my_head = is_wide(layer), layer // 2

    def visit(step):
        return (
            layer,
            layer + 1 - 2 * lax.rem(layer, 2),
            lax.rem(layer + 2, layers),
            layers - 1 - layer,
        )[step]

    def piece(kind, target):
        head = target // 2
        value = pl.ds(head * lanes, lanes)
        if not is_wide(target):
            return (key_narrow_ref, None, value_narrow_ref, query_narrow_ref, None)[kind].at[:, value]
        if kind == 2:
            return value_wide_ref.at[:, value]
        ref = key_wide_ref if kind < 2 else query_wide_ref
        return ref.at[:, pl.ds((2 * head + kind % 3) * lanes, lanes)]

    def place(kind, index, half):
        row = 2 * index + half if kind < 3 else index
        at = pl.ds(pl.multiple_of(row * tok_rows, tok_rows), tok_rows)
        if kind == 2:
            return value_all.at[at, pl.ds(0, lanes)]
        return key_all.at[kind, at, :] if kind < 2 else query_all.at[kind - 3, at, :]

    def when_mine(kind, action):
        if kind in (1, 4):
            pl.when(wide == 1)(action)
        else:
            action()

    def to_layer(kind, target):
        return pltpu.make_async_remote_copy(
            src_ref=piece(kind, target),
            dst_ref=place(kind, layer, side),
            send_sem=send_sem.at[kind, target],
            recv_sem=recv_sem.at[kind, layer],
            device_id={"sp": 2 * target + side},
            device_id_type=pl.DeviceIdType.MESH,
        )

    def kinds_for(target, kinds):
        return [kind for kind in kinds if is_wide(target) or kind not in (1, 4)]

    peers = [{"sp": partner}]
    for step in range(1, layers):
        peers.append({"sp": 2 * visit(step) + side})
    for step in range(layers):
        for turn in range(1, ranks):
            peers.append({"sp": 2 * visit(step) + side, "tp": lax.rem(rank + turn, ranks)})
    greet(peers)

    order = sorted(range(layers), key=lambda index: -is_wide(index))
    for kinds in ((0, 1, 2), (3, 4)):
        for target in order if kinds[0] == 0 else reversed(order):
            for kind in kinds_for(target, kinds):

                @pl.when(layer != target)
                def _():
                    to_layer(kind, target).start()

                @pl.when(layer == target)
                def _():
                    pltpu.make_async_copy(
                        piece(kind, target), place(kind, target, side), recv_sem.at[kind, target]
                    ).start()

    value_all[:, lanes:] = jnp.ones((value_all.shape[0], lanes), jnp.bfloat16)

    def landed_here(kind, index, half, sem):
        where = place(kind, index, half)
        pltpu.make_async_copy(where, where, sem.at[kind, index]).wait()

    def pass_on(kind, index):
        where = place(kind, index, side)
        return pltpu.make_async_remote_copy(
            src_ref=where,
            dst_ref=where,
            send_sem=pass_send.at[kind, index],
            recv_sem=pass_recv.at[kind, index],
            device_id={"sp": partner},
            device_id_type=pl.DeviceIdType.MESH,
        )

    for step in range(layers):
        index = visit(step)
        for kind in range(3):

            def forward():
                landed_here(kind, index, side, recv_sem)
                pass_on(kind, index).start()

            when_mine(kind, forward)
    for step in range(layers):
        index = visit(step)
        for kind in range(3):
            when_mine(kind, lambda: landed_here(kind, index, 1 - side, pass_recv))

    scale = math.log2(math.e) * jnp.where(wide == 1, lanes ** (-0.5), narrow_size ** (-0.5))
    scale = scale.astype(jnp.float32)
    subtract = jnp.where(wide == 1, wide_sub_ref[my_head], narrow_sub_ref[my_head])
    column = wide * (head_count * ranks) + rank * head_count + my_head

    def to_tokens(index, part):
        row = pl.multiple_of(index * tok_rows + part * out_rows, out_rows)
        source = own.at[pl.ds(row, out_rows), :]
        there = landed.at[:, pl.ds(pl.multiple_of(column * lanes, lanes), lanes)]
        block = 2 * index + side
        remote = pltpu.make_async_remote_copy(
            src_ref=source,
            dst_ref=there,
            send_sem=out_send.at[index, part],
            recv_sem=out_recv.at[column],
            device_id={"sp": block, "tp": part},
            device_id_type=pl.DeviceIdType.MESH,
        )
        here = pltpu.make_async_copy(source, there, out_recv.at[column])
        return remote, here, (block == me) & (rank == part)

    lane = lax.broadcasted_iota(jnp.int32, (tok_rows, lanes), 1)
    for step in range(layers):
        index = visit(step)
        for kind in (3, 4):
            when_mine(kind, lambda: landed_here(kind, index, side, recv_sem))
        at = pl.ds(pl.multiple_of(index * tok_rows, tok_rows), tok_rows)
        mapped = []
        for part in range(2):
            low = jnp.where(wide == 1, 0, part * narrow_size)
            high = jnp.where(wide == 1, lanes, (part + 1) * narrow_size)
            plane = part * wide
            queries = jnp.where(
                (lane >= low) & (lane < high), query_all[plane, at, :].astype(jnp.float32), 0.0
            ).astype(jnp.bfloat16)
            scores = lax.dot_general(
                queries,
                key_all[plane],
                (((1,), (1,)), ((), ())),
                preferred_element_type=jnp.float32,
            )
            top = jnp.max(scores, -1, keepdims=True)
            expo = jnp.exp2(scores * scale - top * scale).astype(jnp.bfloat16)
            summed = jnp.dot(expo, value_all[...], preferred_element_type=jnp.float32)
            mapped.append(summed[:, :lanes] / summed[:, lanes:])
        diff = mapped[0] - subtract * mapped[1]
        normed = diff * lax.rsqrt(jnp.mean(diff * diff, -1, keepdims=True) + 1e-06) * gain_ref[...]
        own[at, :] = normed.astype(jnp.bfloat16)
        for part in range(ranks):
            remote, here, mine = to_tokens(index, part)

            @pl.when(mine)
            def _():
                here.start()

            @pl.when(jnp.logical_not(mine))
            def _():
                remote.start()

    for target in range(layers):
        for kind in kinds_for(target, range(5)):

            @pl.when(layer != target)
            def _():
                to_layer(kind, target).wait_send()

    for index in range(layers):
        for kind in range(3):
            when_mine(kind, lambda: pass_on(kind, index).wait_send())
        for part in range(ranks):
            remote, here, mine = to_tokens(index, part)

            @pl.when(jnp.logical_not(mine))
            def _():
                remote.wait_send()

    for head in range(layers * ranks):
        where = landed.at[:, pl.ds(head * lanes, lanes)]
        pltpu.make_async_copy(where, where, out_recv.at[head]).wait()
    out_ref[...] = landed[...]


def attend_by_head(queries, keys, values, subtract_narrow, subtract_wide, head_gain, out_rows):
    shards, ranks = lax.axis_size("sp"), lax.axis_size("tp")
    head_count, lanes = subtract_narrow.shape[0], head_gain.shape[0]
    tok_rows = keys[0].shape[0]
    tokens, layers = shards * tok_rows, 2 * head_count
    heads = layers * ranks
    vmem = pl.BlockSpec(memory_space=pltpu.VMEM)
    smem = pl.BlockSpec(memory_space=pltpu.SMEM)
    dma = pltpu.SemaphoreType.DMA
    return pl.pallas_call(
        attend_kernel,
        out_shape=jax.ShapeDtypeStruct((out_rows, heads * lanes), jnp.bfloat16),
        in_specs=[smem, smem, vmem] + [pl.BlockSpec(memory_space=pl.ANY)] * 6,
        out_specs=vmem,
        scratch_shapes=[
            pltpu.VMEM((2, layers * tok_rows, lanes), jnp.bfloat16),
            pltpu.VMEM((2, tokens, lanes), jnp.bfloat16),
            pltpu.VMEM((tokens, 2 * lanes), jnp.bfloat16),
            pltpu.VMEM((layers * tok_rows, lanes), jnp.bfloat16),
            pltpu.VMEM((out_rows, heads * lanes), jnp.bfloat16),
            dma((5, layers)),
            dma((5, layers)),
            dma((3, layers)),
            dma((3, layers)),
            dma((layers, ranks)),
            dma((heads,)),
        ],
        compiler_params=pltpu.CompilerParams(
            collective_id=0, has_side_effects=True, vmem_limit_bytes=62 * 1024 * 1024
        ),
    )(
        subtract_narrow,
        subtract_wide,
        head_gain[None],
        queries[0],
        keys[0],
        values[0],
        queries[1],
        keys[1],
        values[1],
    )


def head_split_fits(tok_rows, out_rows, ranks, heads, shards, value_size, key_sizes):
    return (
        heads == 2
        and shards == 4 * heads
        and out_rows * ranks == tok_rows
        and tok_rows % 16 == 0
        and out_rows % 16 == 0
        and value_size == 128
        and key_sizes == (value_size // 2, value_size)
    )


def flip(index, bits, size):
    flipped, bit = 0, 1
    while bit < size:
        one, other = lax.rem(index // bit, 2), lax.rem(bits // bit, 2)
        flipped = flipped + bit * (one + other - 2 * one * other)
        bit *= 2
    return flipped


def expert_kernel(
    send_ref,
    gate_from,
    up_from,
    down_from,
    out_ref,
    gate_ref,
    up_ref,
    down_ref,
    weight_sem,
    rows,
    part,
    pairs,
    mid,
    cross,
    done,
    back,
    far_send,
    far_recv,
    near_send,
    near_recv,
    sum_send,
    sum_recv,
    back_send,
    back_recv,
):
    shards, ranks = lax.axis_size("sp"), lax.axis_size("tp")
    me, rank = lax.axis_index("sp"), lax.axis_index("tp")
    cap = send_ref.shape[0] // shards
    side, core = rank // 2, lax.rem(rank, 2)
    partner, across = rank + 1 - 2 * core, lax.rem(rank + 2, ranks)
    my_place, far_place = core * 2 + side, core * 2 + 1 - side
    block = ranks * cap

    def at(ref, index, count=1):
        return ref.at[pl.ds(pl.multiple_of(index * cap, cap), count * cap), :]

    def copy_to(source, place, send, recv, device):
        return pltpu.make_async_remote_copy(
            src_ref=source,
            dst_ref=place,
            send_sem=send,
            recv_sem=recv,
            device_id=device,
            device_id_type=pl.DeviceIdType.MESH,
        )

    def far(hop):
        target = flip(me, hop, shards)
        return copy_to(
            at(send_ref, target),
            at(rows, hop * ranks + my_place),
            far_send.at[hop],
            far_recv.at[hop],
            {"sp": target},
        )

    def near(kind, hop):
        place = far_place if kind == 2 else my_place
        piece = at(rows, hop * ranks + place)
        device = {"tp": across if kind == 1 else partner}
        return copy_to(piece, piece, near_send.at[kind, hop], near_recv.at[kind, hop], device)

    def pair_sum(hop):
        return copy_to(
            at(part, hop * ranks + (1 - core) * 2, 2),
            at(pairs, hop * 2, 2),
            sum_send.at[0, hop],
            sum_recv.at[0, hop],
            {"tp": partner},
        )

    def cross_sum(hop):
        return copy_to(
            at(mid, hop), at(cross, hop), sum_send.at[1, hop], sum_recv.at[1, hop], {"tp": across}
        )

    def give_back(hop):
        return copy_to(
            at(done, hop),
            at(back, me),
            back_send.at[hop],
            back_recv.at[hop],
            {"sp": flip(me, hop, shards)},
        )

    weights = [
        pltpu.make_async_copy(source, place, weight_sem.at[index])
        for index, (source, place) in enumerate(
            zip((gate_from, up_from, down_from), (gate_ref, up_ref, down_ref))
        )
    ]
    for copy in weights:
        copy.start()
    greet(
        [{"tp": partner}, {"tp": across}]
        + [{"sp": flip(me, hop, shards)} for hop in range(1, shards)]
    )

    @pl.loop(1, shards)
    def _(hop):
        far(hop).start()

    own_rows = pltpu.make_async_copy(at(send_ref, me), at(rows, my_place), far_recv.at[0])
    own_rows.start()
    own_rows.wait()

    def share(hop):
        @pl.when(hop > 0)
        def _():
            far(hop).wait_recv()

        near(0, hop).start()
        near(1, hop).start()

    def relay(hop):
        near(1, hop).wait_recv()
        near(2, hop).start()

    def compute(hop):
        @pl.when(hop == 0)
        def _():
            for copy in weights:
                copy.wait()

        near(0, hop).wait_recv()
        near(2, hop).wait_recv()
        span = pl.ds(pl.multiple_of(hop * block, block), block)
        taken = rows[span, :]
        gate = jnp.dot(taken, gate_ref[...], preferred_element_type=jnp.float32)
        up = jnp.dot(taken, up_ref[...], preferred_element_type=jnp.float32)
        inner = (jax.nn.silu(gate) * up).astype(jnp.bfloat16)
        part[span, :] = jnp.dot(inner, down_ref[...], preferred_element_type=jnp.float32).astype(
            jnp.bfloat16
        )
        pair_sum(hop).start()

    def both(hop, place):
        mine = at(part, hop * ranks + core * 2 + place)[...].astype(jnp.float32)
        return mine + at(pairs, hop * 2 + place)[...].astype(jnp.float32)

    def add_pair(hop):
        pair_sum(hop).wait_recv()
        at(mid, hop)[...] = both(hop, 1 - side).astype(jnp.bfloat16)
        cross_sum(hop).start()

    def finish(hop):
        cross_sum(hop).wait_recv()
        total = both(hop, side) + at(cross, hop)[...].astype(jnp.float32)
        at(done, hop)[...] = total.astype(jnp.bfloat16)

        @pl.when(hop > 0)
        def _():
            give_back(hop).start()

    stages = (share, relay, compute, add_pair, finish)

    @pl.loop(0, shards + len(stages) - 1)
    def _(step):
        for late, stage in enumerate(stages):
            hop = step - late

            @pl.when((hop >= 0) & (hop < shards))
            def _():
                stage(hop)

    own_back = pltpu.make_async_copy(at(done, 0), at(back, me), back_recv.at[0])
    own_back.start()
    own_back.wait()

    @pl.loop(0, shards)
    def _(hop):
        for kind in range(3):
            near(kind, hop).wait_send()
        pair_sum(hop).wait_send()
        cross_sum(hop).wait_send()

        @pl.when(hop > 0)
        def _():
            far(hop).wait_send()
            give_back(hop).wait_send()
            give_back(hop).wait_recv()

    out_ref[...] = back[...]


def experts_by_source(outgoing, gate, up, down):
    shards, ranks = lax.axis_size("sp"), lax.axis_size("tp")
    total, width = outgoing.shape
    vmem = pl.BlockSpec(memory_space=pltpu.VMEM)
    dma = pltpu.SemaphoreType.DMA
    return pl.pallas_call(
        expert_kernel,
        out_shape=jax.ShapeDtypeStruct((total, width), jnp.bfloat16),
        in_specs=[vmem] + [pl.BlockSpec(memory_space=pl.ANY)] * 3,
        out_specs=vmem,
        scratch_shapes=[pltpu.VMEM(part.shape, part.dtype) for part in (gate, up, down)]
        + [dma((3,))]
        + [
            pltpu.VMEM((count * total, width), jnp.bfloat16)
            for count in (ranks, ranks, 2, 1, 1, 1, 1)
        ]
        + [
            dma((shards,)),
            dma((shards,)),
            dma((3, shards)),
            dma((3, shards)),
            dma((2, shards)),
            dma((2, shards)),
            dma((shards,)),
            dma((shards,)),
        ],
        compiler_params=pltpu.CompilerParams(
            collective_id=1, has_side_effects=True, vmem_limit_bytes=62 * 1024 * 1024
        ),
    )(outgoing, gate, up, down)


def on_device(
    residual,
    query_narrow,
    key_narrow,
    value_narrow,
    query_wide,
    key_wide,
    value_wide,
    subtract_narrow,
    subtract_wide,
    head_gain,
    out_narrow,
    out_wide,
    norm1_gain,
    norm2_gain,
    expert_ids,
    expert_weight,
    gate_proj,
    up_proj,
    down_proj,
):
    tok_rows = query_narrow.shape[0]
    head_count = subtract_narrow.shape[0]
    value_size = head_gain.shape[0]
    if head_split_fits(
        tok_rows,
        residual.shape[0],
        lax.axis_size("tp"),
        head_count,
        lax.axis_size("sp"),
        value_size,
        tuple(part.shape[1] // (2 * head_count) for part in (key_narrow, key_wide)),
    ):
        attended = attend_by_head(
            (query_narrow, query_wide),
            (key_narrow, key_wide),
            (value_narrow, value_wide),
            subtract_narrow,
            subtract_wide,
            head_gain,
            residual.shape[0],
        )
        full_narrow, full_wide = jnp.split(attended, 2, 1)
    else:
        narrow_queries = query_narrow.reshape(tok_rows, head_count, 2, -1)
        wide_queries = query_wide.reshape(tok_rows, head_count, 2, -1)
        narrow_start = start_carry(head_count, tok_rows, value_size)
        wide_start = start_carry(head_count, tok_rows, value_size)
        narrow_state = absorb_keys(
            narrow_start,
            narrow_queries,
            lax.all_gather(key_narrow, "sp", axis=0, tiled=True),
            lax.all_gather(value_narrow, "sp", axis=0, tiled=True),
            tok_rows,
        )
        wide_state = absorb_keys(
            wide_start,
            wide_queries,
            lax.all_gather(key_wide, "sp", axis=0, tiled=True),
            lax.all_gather(value_wide, "sp", axis=0, tiled=True),
            tok_rows,
        )
        attended_narrow = finish_heads(narrow_state, subtract_narrow, head_gain)
        attended_wide = finish_heads(wide_state, subtract_wide, head_gain)
        full_narrow, full_wide = (
            lax.all_to_all(attended_narrow, "tp", split_axis=0, concat_axis=1, tiled=True),
            lax.all_to_all(attended_wide, "tp", split_axis=0, concat_axis=1, tiled=True),
        )
    mix = jnp.dot(full_narrow, out_narrow, preferred_element_type=jnp.float32) + jnp.dot(
        full_wide, out_wide, preferred_element_type=jnp.float32
    )
    hidden = layer_norm(residual_scale * residual.astype(jnp.float32) + mix, norm1_gain).astype(
        jnp.bfloat16
    )
    local_rows, top_count = expert_ids.shape
    experts = lax.axis_size("sp")
    capacity = max(2, 3 * local_rows * top_count // (2 * experts))
    in_kernel = (
        lax.axis_size("tp") == 4
        and experts & (experts - 1) == 0
        and 4 * experts * capacity * residual.shape[1] < 2**23
    )
    if in_kernel:
        capacity = -(-capacity // 16) * 16
    flat_ids = expert_ids.reshape(-1)
    onehot = (flat_ids[:, None] == jnp.arange(experts, dtype=jnp.int32)[None, :]).astype(jnp.int32)
    before = jnp.cumsum(onehot, 0) - onehot
    position = jnp.sum(before * onehot, 1)
    slots = (flat_ids * capacity + position).reshape(local_rows, top_count)
    dispatch_table = jnp.any(
        jnp.arange(experts * capacity, dtype=jnp.int32)[:, None, None] == slots[None], -1
    ).astype(jnp.bfloat16)
    outgoing = jnp.dot(dispatch_table, hidden, preferred_element_type=jnp.float32).astype(
        jnp.bfloat16
    )
    if in_kernel:
        returned_flat = experts_by_source(outgoing, gate_proj[0], up_proj[0], down_proj[0])
        named = slots[..., None] == jnp.arange(experts * capacity, dtype=jnp.int32)
        combine = jnp.sum(jnp.where(named, expert_weight[..., None], 0.0), 1)
        routed = jnp.dot(
            combine, returned_flat.astype(jnp.float32), precision=lax.Precision.HIGHEST
        )
    else:
        outgoing = outgoing.reshape(experts, capacity, -1)
        gathered = lax.all_gather(
            lax.all_to_all(outgoing, "sp", split_axis=0, concat_axis=0, tiled=True),
            "tp",
            axis=1,
            tiled=True,
        )
        flat_rows = gathered.reshape(-1, gathered.shape[2])
        gate_part = jnp.dot(flat_rows, gate_proj[0], preferred_element_type=jnp.float32)
        up_part = jnp.dot(flat_rows, up_proj[0], preferred_element_type=jnp.float32)
        inner = (jax.nn.silu(gate_part) * up_part).astype(jnp.bfloat16)
        partial_out = jnp.dot(inner, down_proj[0], preferred_element_type=jnp.float32).reshape(
            gathered.shape
        )
        summed = lax.psum_scatter(
            partial_out.astype(jnp.bfloat16), "tp", scatter_dimension=1, tiled=True
        )
        returned = lax.all_to_all(summed, "sp", split_axis=0, concat_axis=0, tiled=True)
        returned_flat = returned.reshape(experts * capacity, -1)
        picked = returned_flat[slots].astype(jnp.float32)
        routed = jnp.sum(expert_weight[..., None] * picked, 1)
    return layer_norm(residual_scale * hidden.astype(jnp.float32) + routed, norm2_gain).astype(
        jnp.bfloat16
    )


def solution(mesh):
    placed = (
        P(("sp", "tp"), None),
        P("sp", "tp"),
        P("sp", "tp"),
        P("sp", "tp"),
        P("sp", "tp"),
        P("sp", "tp"),
        P("sp", "tp"),
        P("tp"),
        P("tp"),
        P(),
        P(),
        P(),
        P(),
        P(),
        P(("sp", "tp"), None),
        P(("sp", "tp"), None),
        P("sp", None, "tp"),
        P("sp", None, "tp"),
        P("sp", "tp", None),
    )
    return jax.shard_map(
        on_device, mesh=mesh, in_specs=placed, out_specs=P(("sp", "tp"), None), check_vma=False
    )
```

```python
import functools
import math

import jax
import jax.numpy as jnp
from jax import lax
from jax.experimental import pallas as pl
from jax.experimental.pallas import tpu as pltpu
from jax.sharding import PartitionSpec as P

residual_scale = 2.0**0.5


def layer_norm(values, gain):
    center = jnp.mean(values, -1, keepdims=True)
    spread = jnp.mean(jnp.square(values - center), -1, keepdims=True)
    return (values - center) * lax.rsqrt(spread + 1e-05) * gain


def block_take(shards, shard_rows):
    take = shards
    for count in range(shards, 0, -1):
        if shards % count == 0 and count * shard_rows >= 512:
            take = count
    return take


def start_carry(head_count, tok_rows, value_size):
    return (
        jnp.full((head_count, 2, tok_rows), -1e30, jnp.float32),
        jnp.zeros((head_count, 2, tok_rows), jnp.float32),
        jnp.zeros((head_count, 2, tok_rows, value_size), jnp.float32),
    )


def absorb_keys(carry, queries, key_piece, value_piece, shard_rows):
    head_count = queries.shape[1]
    key_size = queries.shape[3]
    shards = key_piece.shape[0] // shard_rows
    take = block_take(shards, shard_rows)
    span = take * shard_rows

    def one_block(step_index, state):
        rowtop, total, summed = state
        key_block = lax.dynamic_slice_in_dim(key_piece, step_index * span, span, 0).reshape(
            span, head_count, 2, key_size
        )
        value_block = lax.dynamic_slice_in_dim(value_piece, step_index * span, span, 0).reshape(
            span, head_count, -1
        )
        scores = jnp.einsum(
            "qhmd,khmd->hmqk", queries, key_block, preferred_element_type=jnp.float32
        ) * key_size ** (-0.5)
        newtop = jnp.maximum(rowtop, jnp.max(scores, -1))
        shrink = jnp.exp(rowtop - newtop)
        expo = jnp.exp(scores - newtop[..., None])
        total = total * shrink + jnp.sum(expo, -1)
        summed = summed * shrink[..., None] + jnp.einsum(
            "hmqk,khe->hmqe",
            expo.astype(jnp.bfloat16),
            value_block,
            preferred_element_type=jnp.float32,
        )
        return (newtop, total, summed)

    return lax.fori_loop(0, shards // take, one_block, carry)


def finish_heads(carry, subtract, head_gain):
    rowtop, total, summed = carry
    mapped = summed / total[..., None]
    diff = mapped[:, 0] - subtract[:, None, None] * mapped[:, 1]
    normed = diff * lax.rsqrt(jnp.mean(diff * diff, -1, keepdims=True) + 1e-06) * head_gain
    return jnp.transpose(normed, (1, 0, 2)).reshape(diff.shape[1], -1).astype(jnp.bfloat16)


def greet(peers):
    barrier = pltpu.get_barrier_semaphore()
    for peer in peers:
        pl.semaphore_signal(
            barrier, inc=1, device_id=peer, device_id_type=pl.DeviceIdType.MESH
        )
    pl.semaphore_wait(barrier, len(peers))


def attend_part(
    meanwhile,
    narrow_sub_ref,
    wide_sub_ref,
    gain_ref,
    query_narrow_ref,
    key_narrow_ref,
    value_narrow_ref,
    query_wide_ref,
    key_wide_ref,
    value_wide_ref,
    query_all,
    key_all,
    value_all,
    own,
    landed,
    send_sem,
    recv_sem,
    pass_send,
    pass_recv,
    out_send,
    out_recv,
):
    ranks = lax.axis_size("tp")
    me, rank = lax.axis_index("sp"), lax.axis_index("tp")
    layer, side = me // 2, lax.rem(me, 2)
    partner = me + 1 - 2 * side
    tok_rows = key_narrow_ref.shape[0]
    head_count = narrow_sub_ref.shape[0]
    layers = 2 * head_count
    out_rows, lanes = landed.shape[0], gain_ref.shape[1]
    narrow_size = lanes // 2

    def is_wide(index):
        return lax.rem((index + 1) // 2, 2) if not isinstance(index, int) else (index + 1) // 2 % 2

    wide, my_head = is_wide(layer), layer // 2

    def visit(step):
        return (
            layer,
            layer + 1 - 2 * lax.rem(layer, 2),
            lax.rem(layer + 2, layers),
            layers - 1 - layer,
        )[step]

    def piece(kind, target):
        head = target // 2
        value = pl.ds(head * lanes, lanes)
        if not is_wide(target):
            return (key_narrow_ref, None, value_narrow_ref, query_narrow_ref, None)[kind].at[:, value]
        if kind == 2:
            return value_wide_ref.at[:, value]
        ref = key_wide_ref if kind < 2 else query_wide_ref
        return ref.at[:, pl.ds((2 * head + kind % 3) * lanes, lanes)]

    def place(kind, index, half):
        row = 2 * index + half if kind < 3 else index
        at = pl.ds(pl.multiple_of(row * tok_rows, tok_rows), tok_rows)
        if kind == 2:
            return value_all.at[at, pl.ds(0, lanes)]
        return key_all.at[kind, at, :] if kind < 2 else query_all.at[kind - 3, at, :]

    def when_mine(kind, action):
        if kind in (1, 4):
            pl.when(wide == 1)(action)
        else:
            action()

    def to_layer(kind, target):
        return pltpu.make_async_remote_copy(
            src_ref=piece(kind, target),
            dst_ref=place(kind, layer, side),
            send_sem=send_sem.at[kind, target],
            recv_sem=recv_sem.at[kind, layer],
            device_id={"sp": 2 * target + side},
            device_id_type=pl.DeviceIdType.MESH,
        )

    def kinds_for(target, kinds):
        return [kind for kind in kinds if is_wide(target) or kind not in (1, 4)]

    peers = [{"sp": partner}]
    for step in range(1, layers):
        for column in range(2):
            peers.append({"sp": 2 * visit(step) + column})
    for step in range(layers):
        for turn in range(1, ranks):
            peers.append({"sp": 2 * visit(step) + side, "tp": lax.rem(rank + turn, ranks)})
    greet(peers)

    order = sorted(range(layers), key=lambda index: -is_wide(index))
    for kinds in ((0, 1, 2), (3, 4)):
        for target in order if kinds[0] == 0 else reversed(order):
            for kind in kinds_for(target, kinds):

                @pl.when(layer != target)
                def _():
                    to_layer(kind, target).start()

                @pl.when(layer == target)
                def _():
                    pltpu.make_async_copy(
                        piece(kind, target), place(kind, target, side), recv_sem.at[kind, target]
                    ).start()

    value_all[:, lanes:] = jnp.ones((value_all.shape[0], lanes), jnp.bfloat16)

    meanwhile()

    def landed_here(kind, index, half, sem):
        where = place(kind, index, half)
        pltpu.make_async_copy(where, where, sem.at[kind, index]).wait()

    def pass_on(kind, index):
        where = place(kind, index, side)
        return pltpu.make_async_remote_copy(
            src_ref=where,
            dst_ref=where,
            send_sem=pass_send.at[kind, index],
            recv_sem=pass_recv.at[kind, index],
            device_id={"sp": partner},
            device_id_type=pl.DeviceIdType.MESH,
        )

    for step in range(layers):
        index = visit(step)
        for kind in range(3):

            def forward():
                landed_here(kind, index, side, recv_sem)
                pass_on(kind, index).start()

            when_mine(kind, forward)
    for step in range(layers):
        index = visit(step)
        for kind in range(3):
            when_mine(kind, lambda: landed_here(kind, index, 1 - side, pass_recv))

    scale = math.log2(math.e) * jnp.where(wide == 1, lanes ** (-0.5), narrow_size ** (-0.5))
    scale = scale.astype(jnp.float32)
    subtract = jnp.where(wide == 1, wide_sub_ref[my_head], narrow_sub_ref[my_head])
    column = wide * (head_count * ranks) + rank * head_count + my_head

    def to_tokens(index, part):
        row = pl.multiple_of(index * tok_rows + part * out_rows, out_rows)
        source = own.at[pl.ds(row, out_rows), :]
        there = landed.at[:, pl.ds(pl.multiple_of(column * lanes, lanes), lanes)]
        block = 2 * index + side
        remote = pltpu.make_async_remote_copy(
            src_ref=source,
            dst_ref=there,
            send_sem=out_send.at[index, part],
            recv_sem=out_recv.at[column],
            device_id={"sp": block, "tp": part},
            device_id_type=pl.DeviceIdType.MESH,
        )
        here = pltpu.make_async_copy(source, there, out_recv.at[column])
        return remote, here, (block == me) & (rank == part)

    lane = lax.broadcasted_iota(jnp.int32, (tok_rows, lanes), 1)
    for step in list(range(1, layers)) + [0]:
        index = visit(step)
        for kind in (3, 4):
            when_mine(kind, lambda: landed_here(kind, index, side, recv_sem))
        at = pl.ds(pl.multiple_of(index * tok_rows, tok_rows), tok_rows)
        mapped = []
        for part in range(2):
            low = jnp.where(wide == 1, 0, part * narrow_size)
            high = jnp.where(wide == 1, lanes, (part + 1) * narrow_size)
            plane = part * wide
            queries = jnp.where(
                (lane >= low) & (lane < high), query_all[plane, at, :].astype(jnp.float32), 0.0
            ).astype(jnp.bfloat16)
            scores = lax.dot_general(
                queries,
                key_all[plane],
                (((1,), (1,)), ((), ())),
                preferred_element_type=jnp.float32,
            )
            top = jnp.max(scores, -1, keepdims=True)
            expo = jnp.exp2(scores * scale - top * scale).astype(jnp.bfloat16)
            summed = jnp.dot(expo, value_all[...], preferred_element_type=jnp.float32)
            mapped.append(summed[:, :lanes] / summed[:, lanes:])
        diff = mapped[0] - subtract * mapped[1]
        normed = diff * lax.rsqrt(jnp.mean(diff * diff, -1, keepdims=True) + 1e-06) * gain_ref[...]
        own[at, :] = normed.astype(jnp.bfloat16)
        for part in range(ranks):
            remote, here, mine = to_tokens(index, part)

            @pl.when(mine)
            def _():
                here.start()

            @pl.when(jnp.logical_not(mine))
            def _():
                remote.start()

    for head in range(layers * ranks):
        where = landed.at[:, pl.ds(head * lanes, lanes)]
        pltpu.make_async_copy(where, where, out_recv.at[head]).wait()

    def drain():
        for target in range(layers):
            for kind in kinds_for(target, range(5)):

                @pl.when(layer != target)
                def _():
                    to_layer(kind, target).wait_send()

        for index in range(layers):
            for kind in range(3):
                when_mine(kind, lambda: pass_on(kind, index).wait_send())
            for part in range(ranks):
                remote, here, mine = to_tokens(index, part)

                @pl.when(jnp.logical_not(mine))
                def _():
                    remote.wait_send()

    return drain


def head_split_fits(tok_rows, out_rows, ranks, heads, shards, value_size, key_sizes):
    return (
        heads == 2
        and shards == 4 * heads
        and out_rows * ranks == tok_rows
        and tok_rows % 16 == 0
        and out_rows % 16 == 0
        and value_size == 128
        and key_sizes == (value_size // 2, value_size)
    )


def flip(index, bits, size):
    flipped, bit = 0, 1
    while bit < size:
        one, other = lax.rem(index // bit, 2), lax.rem(bits // bit, 2)
        flipped = flipped + bit * (one + other - 2 * one * other)
        bit *= 2
    return flipped


def expert_part(
    weights,
    send_ref,
    gate_ref,
    up_ref,
    down_ref,
    rows,
    part,
    pairs,
    mid,
    cross,
    done,
    back,
    far_send,
    far_recv,
    near_send,
    near_recv,
    sum_send,
    sum_recv,
    back_send,
    back_recv,
):
    shards, ranks = lax.axis_size("sp"), lax.axis_size("tp")
    me, rank = lax.axis_index("sp"), lax.axis_index("tp")
    cap = send_ref.shape[0] // shards
    side, core = rank // 2, lax.rem(rank, 2)
    partner, across = rank + 1 - 2 * core, lax.rem(rank + 2, ranks)
    my_place, far_place = core * 2 + side, core * 2 + 1 - side
    block = ranks * cap

    def at(ref, index, count=1):
        return ref.at[pl.ds(pl.multiple_of(index * cap, cap), count * cap), :]

    def copy_to(source, place, send, recv, device):
        return pltpu.make_async_remote_copy(
            src_ref=source,
            dst_ref=place,
            send_sem=send,
            recv_sem=recv,
            device_id=device,
            device_id_type=pl.DeviceIdType.MESH,
        )

    def far(hop):
        target = flip(me, hop, shards)
        return copy_to(
            at(send_ref, target),
            at(rows, hop * ranks + my_place),
            far_send.at[hop],
            far_recv.at[hop],
            {"sp": target},
        )

    def near(kind, hop):
        place = far_place if kind == 2 else my_place
        piece = at(rows, hop * ranks + place)
        device = {"tp": across if kind == 1 else partner}
        return copy_to(piece, piece, near_send.at[kind, hop], near_recv.at[kind, hop], device)

    def pair_sum(hop):
        return copy_to(
            at(part, hop * ranks + (1 - core) * 2, 2),
            at(pairs, hop * 2, 2),
            sum_send.at[0, hop],
            sum_recv.at[0, hop],
            {"tp": partner},
        )

    def cross_sum(hop):
        return copy_to(
            at(mid, hop), at(cross, hop), sum_send.at[1, hop], sum_recv.at[1, hop], {"tp": across}
        )

    def give_back(hop):
        return copy_to(
            at(done, hop),
            at(back, me),
            back_send.at[hop],
            back_recv.at[hop],
            {"sp": flip(me, hop, shards)},
        )

    @pl.loop(1, shards)
    def _(hop):
        far(hop).start()

    own_rows = pltpu.make_async_copy(at(send_ref, me), at(rows, my_place), far_recv.at[0])
    own_rows.start()
    own_rows.wait()

    def share(hop):
        @pl.when(hop > 0)
        def _():
            far(hop).wait_recv()

        near(0, hop).start()
        near(1, hop).start()

    def relay(hop):
        near(1, hop).wait_recv()
        near(2, hop).start()

    def compute(hop):
        @pl.when(hop == 0)
        def _():
            for copy in weights:
                copy.wait()

        near(0, hop).wait_recv()
        near(2, hop).wait_recv()
        span = pl.ds(pl.multiple_of(hop * block, block), block)
        taken = rows[span, :]
        gate = jnp.dot(taken, gate_ref[...], preferred_element_type=jnp.float32)
        up = jnp.dot(taken, up_ref[...], preferred_element_type=jnp.float32)
        inner = (jax.nn.silu(gate) * up).astype(jnp.bfloat16)
        part[span, :] = jnp.dot(inner, down_ref[...], preferred_element_type=jnp.float32).astype(
            jnp.bfloat16
        )
        pair_sum(hop).start()

    def both(hop, place):
        mine = at(part, hop * ranks + core * 2 + place)[...].astype(jnp.float32)
        return mine + at(pairs, hop * 2 + place)[...].astype(jnp.float32)

    def add_pair(hop):
        pair_sum(hop).wait_recv()
        at(mid, hop)[...] = both(hop, 1 - side).astype(jnp.bfloat16)
        cross_sum(hop).start()

    def finish(hop):
        cross_sum(hop).wait_recv()
        total = both(hop, side) + at(cross, hop)[...].astype(jnp.float32)
        at(done, hop)[...] = total.astype(jnp.bfloat16)

        @pl.when(hop > 0)
        def _():
            give_back(hop).start()

    stages = (share, relay, compute, add_pair, finish)

    @pl.loop(0, shards + len(stages) - 1)
    def _(step):
        for late, stage in enumerate(stages):
            hop = step - late

            @pl.when((hop >= 0) & (hop < shards))
            def _():
                stage(hop)

    own_back = pltpu.make_async_copy(at(done, 0), at(back, me), back_recv.at[0])
    own_back.start()
    own_back.wait()

    @pl.loop(0, shards)
    def _(hop):
        for kind in range(3):
            near(kind, hop).wait_send()
        pair_sum(hop).wait_send()
        cross_sum(hop).wait_send()

        @pl.when(hop > 0)
        def _():
            far(hop).wait_send()
            give_back(hop).wait_send()
            give_back(hop).wait_recv()


def norm_rows(values):
    center = jnp.mean(values, -1, keepdims=True)
    spread = jnp.mean(jnp.square(values - center), -1, keepdims=True)
    return (values - center) * lax.rsqrt(spread + 1e-05)


def layer_kernel(
    narrow_sub_ref,
    wide_sub_ref,
    gain_ref,
    residual_ref,
    norm1_ref,
    ids_ref,
    choice_ref,
    query_narrow_ref,
    key_narrow_ref,
    value_narrow_ref,
    query_wide_ref,
    key_wide_ref,
    value_wide_ref,
    narrow_from,
    wide_from,
    gate_from,
    up_from,
    down_from,
    out_ref,
    mix_weight,
    gate_ref,
    up_ref,
    down_ref,
    hidden,
    send_ref,
    table,
    combine,
    ids_wide,
    choice_wide,
    mix_sem,
    weight_sem,
    *scratch,
):
    attend_scratch, expert_scratch = scratch[:11], scratch[11:]
    landed = attend_scratch[4]
    back = expert_scratch[6]
    top_count, rows = ids_ref.shape
    columns = table.shape[1]
    experts = lax.axis_size("sp")
    total = send_ref.shape[0]
    capacity = total // experts
    depth = narrow_from.shape[0]

    def fetch(source, place, sem):
        copy = pltpu.make_async_copy(source, place, sem)
        copy.start()
        return copy

    mixers = [
        fetch(narrow_from, mix_weight.at[pl.ds(0, depth), :], mix_sem.at[0]),
        fetch(wide_from, mix_weight.at[pl.ds(depth, depth), :], mix_sem.at[1]),
    ]
    weights = [
        fetch(gate_from, gate_ref, weight_sem.at[0]),
        fetch(up_from, up_ref, weight_sem.at[1]),
        fetch(down_from, down_ref, weight_sem.at[2]),
    ]

    def route():
        ids_wide[...] = jnp.full(ids_wide.shape, -1, jnp.int32)
        ids_wide[:, pl.ds(0, rows)] = ids_ref[...]
        choice_wide[...] = jnp.zeros_like(choice_wide)
        choice_wide[:, pl.ds(0, rows)] = choice_ref[...]
        ids = [ids_wide[pl.ds(choice, 1), :] for choice in range(top_count)]
        expert = lax.broadcasted_iota(jnp.int32, (experts, columns), 0)
        named = [(index == expert).astype(jnp.float32) for index in ids]
        later = lax.broadcasted_iota(jnp.int32, (columns, columns), 0) < lax.broadcasted_iota(
            jnp.int32, (columns, columns), 1
        )
        before = jnp.dot(
            sum(named).astype(jnp.bfloat16),
            later.astype(jnp.float32).astype(jnp.bfloat16),
            preferred_element_type=jnp.float32,
        )
        line = lax.broadcasted_iota(jnp.int32, (total, columns), 0)
        picks = jnp.zeros((total, columns), jnp.float32)
        mixing = jnp.zeros((total, columns), jnp.float32)
        for choice in range(top_count):
            held = jnp.sum(before * named[choice], 0, keepdims=True).astype(jnp.int32)
            taken = (ids[choice] * capacity + held == line) & (ids[choice] >= 0)
            picks = jnp.where(taken, 1.0, picks)
            mixing = jnp.where(taken, choice_wide[pl.ds(choice, 1), :], mixing)
        table[...] = picks.astype(jnp.bfloat16)
        combine[...] = mixing.T
        hidden[...] = jnp.zeros_like(hidden)

    drain = attend_part(
        route,
        narrow_sub_ref,
        wide_sub_ref,
        gain_ref,
        query_narrow_ref,
        key_narrow_ref,
        value_narrow_ref,
        query_wide_ref,
        key_wide_ref,
        value_wide_ref,
        *attend_scratch,
    )
    for copy in mixers:
        copy.wait()
    mix = jnp.dot(landed[...], mix_weight[...], preferred_element_type=jnp.float32)
    held = residual_scale * residual_ref[...].astype(jnp.float32) + mix
    hidden[pl.ds(0, rows), :] = (norm_rows(held) * norm1_ref[...]).astype(jnp.bfloat16)
    send_ref[...] = jnp.dot(
        table[...], hidden[...], preferred_element_type=jnp.float32
    ).astype(jnp.bfloat16)
    expert_part(weights, send_ref, gate_ref, up_ref, down_ref, *expert_scratch)
    coarse = combine[...].astype(jnp.bfloat16)
    fine = (combine[...] - coarse.astype(jnp.float32)).astype(jnp.bfloat16)
    routed = jnp.dot(coarse, back[...], preferred_element_type=jnp.float32) + jnp.dot(
        fine, back[...], preferred_element_type=jnp.float32
    )
    tokens = residual_scale * hidden[pl.ds(0, rows), :].astype(jnp.float32) + routed[:rows]
    out_ref[...] = norm_rows(tokens)
    drain()


def whole_layer(
    residual,
    attend_args,
    subtract_narrow,
    subtract_wide,
    head_gain,
    out_weights,
    norm1_gain,
    norm2_gain,
    expert_ids,
    expert_weight,
    expert_weights,
    capacity,
):
    shards, ranks = lax.axis_size("sp"), lax.axis_size("tp")
    head_count, lanes = subtract_narrow.shape[0], head_gain.shape[0]
    tok_rows = attend_args[0].shape[0]
    rows, width = residual.shape
    tokens, layers = shards * tok_rows, 2 * head_count
    heads = layers * ranks
    total = shards * capacity
    vmem = pl.BlockSpec(memory_space=pltpu.VMEM)
    smem = pl.BlockSpec(memory_space=pltpu.SMEM)
    dma = pltpu.SemaphoreType.DMA

    def buffer(*shape):
        return pltpu.VMEM(shape, jnp.bfloat16)

    columns = -(-rows // 128) * 128
    normed = pl.pallas_call(
        layer_kernel,
        out_shape=jax.ShapeDtypeStruct((rows, width), jnp.float32),
        in_specs=[smem, smem] + [vmem] * 5 + [pl.BlockSpec(memory_space=pl.ANY)] * 11,
        out_specs=vmem,
        scratch_shapes=[buffer(heads * lanes, width)]
        + [buffer(*part.shape) for part in expert_weights]
        + [
            buffer(columns, width),
            buffer(total, width),
            buffer(total, columns),
            pltpu.VMEM((columns, total), jnp.float32),
            pltpu.VMEM(expert_ids.shape[1:] + (columns,), jnp.int32),
            pltpu.VMEM(expert_ids.shape[1:] + (columns,), jnp.float32),
            dma((2,)),
            dma((3,)),
            buffer(2, layers * tok_rows, lanes),
            buffer(2, tokens, lanes),
            buffer(tokens, 2 * lanes),
            buffer(layers * tok_rows, lanes),
            buffer(rows, heads * lanes),
            dma((5, layers)),
            dma((5, layers)),
            dma((3, layers)),
            dma((3, layers)),
            dma((layers, ranks)),
            dma((heads,)),
        ]
        + [buffer(count * total, width) for count in (ranks, ranks, 2, 1, 1, 1, 1)]
        + [
            dma((shards,)),
            dma((shards,)),
            dma((3, shards)),
            dma((3, shards)),
            dma((2, shards)),
            dma((2, shards)),
            dma((shards,)),
            dma((shards,)),
        ],
        compiler_params=pltpu.CompilerParams(
            collective_id=0, has_side_effects=True, vmem_limit_bytes=62 * 1024 * 1024
        ),
    )(
        subtract_narrow,
        subtract_wide,
        head_gain[None],
        residual,
        norm1_gain[None],
        expert_ids.T,
        expert_weight.T,
        *attend_args,
        *out_weights,
        *expert_weights,
    )
    return (normed * norm2_gain).astype(jnp.bfloat16)


def on_device(
    residual,
    query_narrow,
    key_narrow,
    value_narrow,
    query_wide,
    key_wide,
    value_wide,
    subtract_narrow,
    subtract_wide,
    head_gain,
    out_narrow,
    out_wide,
    norm1_gain,
    norm2_gain,
    expert_ids,
    expert_weight,
    gate_proj,
    up_proj,
    down_proj,
):
    tok_rows = query_narrow.shape[0]
    head_count = subtract_narrow.shape[0]
    value_size = head_gain.shape[0]
    local_rows, top_count = expert_ids.shape
    experts = lax.axis_size("sp")
    capacity = max(2, 3 * local_rows * top_count // (2 * experts))
    padded = -(-capacity // 16) * 16
    if (
        head_split_fits(
            tok_rows,
            local_rows,
            lax.axis_size("tp"),
            head_count,
            experts,
            value_size,
            tuple(part.shape[1] // (2 * head_count) for part in (key_narrow, key_wide)),
        )
        and lax.axis_size("tp") == 4
        and top_count == 2
        and experts & (experts - 1) == 0
        and 4 * experts * padded * residual.shape[1] < 2**23
    ):
        return whole_layer(
            residual,
            (query_narrow, key_narrow, value_narrow, query_wide, key_wide, value_wide),
            subtract_narrow,
            subtract_wide,
            head_gain,
            (out_narrow, out_wide),
            norm1_gain,
            norm2_gain,
            expert_ids,
            expert_weight,
            (gate_proj[0], up_proj[0], down_proj[0]),
            padded,
        )
    narrow_queries = query_narrow.reshape(tok_rows, head_count, 2, -1)
    wide_queries = query_wide.reshape(tok_rows, head_count, 2, -1)
    narrow_start = start_carry(head_count, tok_rows, value_size)
    wide_start = start_carry(head_count, tok_rows, value_size)
    narrow_state = absorb_keys(
        narrow_start,
        narrow_queries,
        lax.all_gather(key_narrow, "sp", axis=0, tiled=True),
        lax.all_gather(value_narrow, "sp", axis=0, tiled=True),
        tok_rows,
    )
    wide_state = absorb_keys(
        wide_start,
        wide_queries,
        lax.all_gather(key_wide, "sp", axis=0, tiled=True),
        lax.all_gather(value_wide, "sp", axis=0, tiled=True),
        tok_rows,
    )
    attended_narrow = finish_heads(narrow_state, subtract_narrow, head_gain)
    attended_wide = finish_heads(wide_state, subtract_wide, head_gain)
    full_narrow, full_wide = (
        lax.all_to_all(attended_narrow, "tp", split_axis=0, concat_axis=1, tiled=True),
        lax.all_to_all(attended_wide, "tp", split_axis=0, concat_axis=1, tiled=True),
    )
    mix = jnp.dot(full_narrow, out_narrow, preferred_element_type=jnp.float32) + jnp.dot(
        full_wide, out_wide, preferred_element_type=jnp.float32
    )
    hidden = layer_norm(residual_scale * residual.astype(jnp.float32) + mix, norm1_gain).astype(
        jnp.bfloat16
    )
    flat_ids = expert_ids.reshape(-1)
    onehot = (flat_ids[:, None] == jnp.arange(experts, dtype=jnp.int32)[None, :]).astype(jnp.int32)
    before = jnp.cumsum(onehot, 0) - onehot
    position = jnp.sum(before * onehot, 1)
    slots = (flat_ids * capacity + position).reshape(local_rows, top_count)
    dispatch_table = jnp.any(
        jnp.arange(experts * capacity, dtype=jnp.int32)[:, None, None] == slots[None], -1
    ).astype(jnp.bfloat16)
    outgoing = jnp.dot(dispatch_table, hidden, preferred_element_type=jnp.float32).astype(
        jnp.bfloat16
    )
    outgoing = outgoing.reshape(experts, capacity, -1)
    gathered = lax.all_gather(
        lax.all_to_all(outgoing, "sp", split_axis=0, concat_axis=0, tiled=True),
        "tp",
        axis=1,
        tiled=True,
    )
    flat_rows = gathered.reshape(-1, gathered.shape[2])
    gate_part = jnp.dot(flat_rows, gate_proj[0], preferred_element_type=jnp.float32)
    up_part = jnp.dot(flat_rows, up_proj[0], preferred_element_type=jnp.float32)
    inner = (jax.nn.silu(gate_part) * up_part).astype(jnp.bfloat16)
    partial_out = jnp.dot(inner, down_proj[0], preferred_element_type=jnp.float32).reshape(
        gathered.shape
    )
    summed = lax.psum_scatter(
        partial_out.astype(jnp.bfloat16), "tp", scatter_dimension=1, tiled=True
    )
    returned = lax.all_to_all(summed, "sp", split_axis=0, concat_axis=0, tiled=True)
    returned_flat = returned.reshape(experts * capacity, -1)
    picked = returned_flat[slots].astype(jnp.float32)
    routed = jnp.sum(expert_weight[..., None] * picked, 1)
    return layer_norm(residual_scale * hidden.astype(jnp.float32) + routed, norm2_gain).astype(
        jnp.bfloat16
    )


def solution(mesh):
    placed = (
        P(("sp", "tp"), None),
        P("sp", "tp"),
        P("sp", "tp"),
        P("sp", "tp"),
        P("sp", "tp"),
        P("sp", "tp"),
        P("sp", "tp"),
        P("tp"),
        P("tp"),
        P(),
        P(),
        P(),
        P(),
        P(),
        P(("sp", "tp"), None),
        P(("sp", "tp"), None),
        P("sp", None, "tp"),
        P("sp", None, "tp"),
        P("sp", "tp", None),
    )
    return jax.shard_map(
        on_device, mesh=mesh, in_specs=placed, out_specs=P(("sp", "tp"), None), check_vma=False
    )
```

```python
import functools
import math

import jax
import jax.numpy as jnp
from jax import lax
from jax.experimental import pallas as pl
from jax.experimental.pallas import tpu as pltpu
from jax.sharding import PartitionSpec as P

residual_scale = 2.0**0.5


def layer_norm(values, gain):
    center = jnp.mean(values, -1, keepdims=True)
    spread = jnp.mean(jnp.square(values - center), -1, keepdims=True)
    return (values - center) * lax.rsqrt(spread + 1e-05) * gain


def block_take(shards, shard_rows):
    take = shards
    for count in range(shards, 0, -1):
        if shards % count == 0 and count * shard_rows >= 512:
            take = count
    return take


def start_carry(head_count, tok_rows, value_size):
    return (
        jnp.full((head_count, 2, tok_rows), -1e30, jnp.float32),
        jnp.zeros((head_count, 2, tok_rows), jnp.float32),
        jnp.zeros((head_count, 2, tok_rows, value_size), jnp.float32),
    )


def absorb_keys(carry, queries, key_piece, value_piece, shard_rows):
    head_count = queries.shape[1]
    key_size = queries.shape[3]
    shards = key_piece.shape[0] // shard_rows
    take = block_take(shards, shard_rows)
    span = take * shard_rows

    def one_block(step_index, state):
        rowtop, total, summed = state
        key_block = lax.dynamic_slice_in_dim(key_piece, step_index * span, span, 0).reshape(
            span, head_count, 2, key_size
        )
        value_block = lax.dynamic_slice_in_dim(value_piece, step_index * span, span, 0).reshape(
            span, head_count, -1
        )
        scores = jnp.einsum(
            "qhmd,khmd->hmqk", queries, key_block, preferred_element_type=jnp.float32
        ) * key_size ** (-0.5)
        newtop = jnp.maximum(rowtop, jnp.max(scores, -1))
        shrink = jnp.exp(rowtop - newtop)
        expo = jnp.exp(scores - newtop[..., None])
        total = total * shrink + jnp.sum(expo, -1)
        summed = summed * shrink[..., None] + jnp.einsum(
            "hmqk,khe->hmqe",
            expo.astype(jnp.bfloat16),
            value_block,
            preferred_element_type=jnp.float32,
        )
        return (newtop, total, summed)

    return lax.fori_loop(0, shards // take, one_block, carry)


def finish_heads(carry, subtract, head_gain):
    rowtop, total, summed = carry
    mapped = summed / total[..., None]
    diff = mapped[:, 0] - subtract[:, None, None] * mapped[:, 1]
    normed = diff * lax.rsqrt(jnp.mean(diff * diff, -1, keepdims=True) + 1e-06) * head_gain
    return jnp.transpose(normed, (1, 0, 2)).reshape(diff.shape[1], -1).astype(jnp.bfloat16)


def greet(peers):
    barrier = pltpu.get_barrier_semaphore()
    for peer in peers:
        pl.semaphore_signal(
            barrier, inc=1, device_id=peer, device_id_type=pl.DeviceIdType.MESH
        )
    pl.semaphore_wait(barrier, len(peers))


def attend_part(
    meanwhile,
    narrow_sub_ref,
    wide_sub_ref,
    gain_ref,
    query_narrow_ref,
    key_narrow_ref,
    value_narrow_ref,
    query_wide_ref,
    key_wide_ref,
    value_wide_ref,
    query_all,
    key_all,
    value_all,
    own,
    landed,
    send_sem,
    recv_sem,
    pass_send,
    pass_recv,
    out_send,
    out_recv,
):
    ranks = lax.axis_size("tp")
    me, rank = lax.axis_index("sp"), lax.axis_index("tp")
    layer, side = me // 2, lax.rem(me, 2)
    partner = me + 1 - 2 * side
    tok_rows = key_narrow_ref.shape[0]
    head_count = narrow_sub_ref.shape[0]
    layers = 2 * head_count
    out_rows, lanes = landed.shape[0], gain_ref.shape[1]
    narrow_size = lanes // 2

    def is_wide(index):
        return lax.rem((index + 1) // 2, 2) if not isinstance(index, int) else (index + 1) // 2 % 2

    wide, my_head = is_wide(layer), layer // 2

    def visit(step):
        return (
            layer,
            layer + 1 - 2 * lax.rem(layer, 2),
            lax.rem(layer + 2, layers),
            layers - 1 - layer,
        )[step]

    def piece(kind, target):
        head = target // 2
        value = pl.ds(head * lanes, lanes)
        if not is_wide(target):
            return (key_narrow_ref, None, value_narrow_ref, query_narrow_ref, None)[kind].at[:, value]
        if kind == 2:
            return value_wide_ref.at[:, value]
        ref = key_wide_ref if kind < 2 else query_wide_ref
        return ref.at[:, pl.ds((2 * head + kind % 3) * lanes, lanes)]

    def place(kind, index, half):
        row = 2 * index + half if kind < 3 else index
        at = pl.ds(pl.multiple_of(row * tok_rows, tok_rows), tok_rows)
        if kind == 2:
            return value_all.at[at, pl.ds(0, lanes)]
        return key_all.at[kind, at, :] if kind < 2 else query_all.at[kind - 3, at, :]

    def when_mine(kind, action):
        if kind in (1, 4):
            pl.when(wide == 1)(action)
        else:
            action()

    def to_layer(kind, target):
        return pltpu.make_async_remote_copy(
            src_ref=piece(kind, target),
            dst_ref=place(kind, layer, side),
            send_sem=send_sem.at[kind, target],
            recv_sem=recv_sem.at[kind, layer],
            device_id={"sp": 2 * target + side},
            device_id_type=pl.DeviceIdType.MESH,
        )

    def kinds_for(target, kinds):
        return [kind for kind in kinds if is_wide(target) or kind not in (1, 4)]

    peers = [{"sp": partner}]
    for step in range(1, layers):
        for column in range(2):
            peers.append({"sp": 2 * visit(step) + column})
    for step in range(layers):
        for turn in range(1, ranks):
            peers.append({"sp": 2 * visit(step) + side, "tp": lax.rem(rank + turn, ranks)})
    greet(peers)

    order = sorted(range(layers), key=lambda index: -is_wide(index))
    for kinds in ((0, 1, 2), (3, 4)):
        for target in order if kinds[0] == 0 else reversed(order):
            for kind in kinds_for(target, kinds):

                @pl.when(layer != target)
                def _():
                    to_layer(kind, target).start()

                @pl.when(layer == target)
                def _():
                    pltpu.make_async_copy(
                        piece(kind, target), place(kind, target, side), recv_sem.at[kind, target]
                    ).start()

    value_all[:, lanes:] = jnp.ones((value_all.shape[0], lanes), jnp.bfloat16)

    meanwhile()

    def landed_here(kind, index, half, sem):
        where = place(kind, index, half)
        pltpu.make_async_copy(where, where, sem.at[kind, index]).wait()

    def pass_on(kind, index):
        where = place(kind, index, side)
        return pltpu.make_async_remote_copy(
            src_ref=where,
            dst_ref=where,
            send_sem=pass_send.at[kind, index],
            recv_sem=pass_recv.at[kind, index],
            device_id={"sp": partner},
            device_id_type=pl.DeviceIdType.MESH,
        )

    for step in range(layers):
        index = visit(step)
        for kind in range(3):

            def forward():
                landed_here(kind, index, side, recv_sem)
                pass_on(kind, index).start()

            when_mine(kind, forward)
    for step in range(layers):
        index = visit(step)
        for kind in range(3):
            when_mine(kind, lambda: landed_here(kind, index, 1 - side, pass_recv))

    scale = math.log2(math.e) * jnp.where(wide == 1, lanes ** (-0.5), narrow_size ** (-0.5))
    scale = scale.astype(jnp.float32)
    subtract = jnp.where(wide == 1, wide_sub_ref[my_head], narrow_sub_ref[my_head])
    column = wide * (head_count * ranks) + rank * head_count + my_head

    def to_tokens(index, part):
        row = pl.multiple_of(index * tok_rows + part * out_rows, out_rows)
        source = own.at[pl.ds(row, out_rows), :]
        there = landed.at[:, pl.ds(pl.multiple_of(column * lanes, lanes), lanes)]
        block = 2 * index + side
        remote = pltpu.make_async_remote_copy(
            src_ref=source,
            dst_ref=there,
            send_sem=out_send.at[index, part],
            recv_sem=out_recv.at[column],
            device_id={"sp": block, "tp": part},
            device_id_type=pl.DeviceIdType.MESH,
        )
        here = pltpu.make_async_copy(source, there, out_recv.at[column])
        return remote, here, (block == me) & (rank == part)

    lane = lax.broadcasted_iota(jnp.int32, (tok_rows, lanes), 1)
    for step in list(range(1, layers)) + [0]:
        index = visit(step)
        for kind in (3, 4):
            when_mine(kind, lambda: landed_here(kind, index, side, recv_sem))
        at = pl.ds(pl.multiple_of(index * tok_rows, tok_rows), tok_rows)
        mapped = []
        for part in range(2):
            low = jnp.where(wide == 1, 0, part * narrow_size)
            high = jnp.where(wide == 1, lanes, (part + 1) * narrow_size)
            plane = part * wide
            queries = jnp.where(
                (lane >= low) & (lane < high), query_all[plane, at, :].astype(jnp.float32), 0.0
            ).astype(jnp.bfloat16)
            scores = lax.dot_general(
                queries,
                key_all[plane],
                (((1,), (1,)), ((), ())),
                preferred_element_type=jnp.float32,
            )
            top = jnp.max(scores, -1, keepdims=True)
            expo = jnp.exp2(scores * scale - top * scale).astype(jnp.bfloat16)
            summed = jnp.dot(expo, value_all[...], preferred_element_type=jnp.float32)
            mapped.append(summed[:, :lanes] / summed[:, lanes:])
        diff = mapped[0] - subtract * mapped[1]
        normed = diff * lax.rsqrt(jnp.mean(diff * diff, -1, keepdims=True) + 1e-06) * gain_ref[...]
        own[at, :] = normed.astype(jnp.bfloat16)
        for part in range(ranks):
            remote, here, mine = to_tokens(index, part)

            @pl.when(mine)
            def _():
                here.start()

            @pl.when(jnp.logical_not(mine))
            def _():
                remote.start()

    for head in range(layers * ranks):
        where = landed.at[:, pl.ds(head * lanes, lanes)]
        pltpu.make_async_copy(where, where, out_recv.at[head]).wait()

    def drain():
        for target in range(layers):
            for kind in kinds_for(target, range(5)):

                @pl.when(layer != target)
                def _():
                    to_layer(kind, target).wait_send()

        for index in range(layers):
            for kind in range(3):
                when_mine(kind, lambda: pass_on(kind, index).wait_send())
            for part in range(ranks):
                remote, here, mine = to_tokens(index, part)

                @pl.when(jnp.logical_not(mine))
                def _():
                    remote.wait_send()

    return drain


def head_split_fits(tok_rows, out_rows, ranks, heads, shards, value_size, key_sizes):
    return (
        heads == 2
        and shards == 4 * heads
        and out_rows * ranks == tok_rows
        and tok_rows % 16 == 0
        and out_rows % 16 == 0
        and value_size == 128
        and key_sizes == (value_size // 2, value_size)
    )


def hop_bits(hop):
    return 4 * lax.rem(hop, 2) + 2 * lax.rem(hop // 2, 2) + hop // 4


def flip(index, bits, size):
    flipped, bit = 0, 1
    while bit < size:
        one, other = lax.rem(index // bit, 2), lax.rem(bits // bit, 2)
        flipped = flipped + bit * (one + other - 2 * one * other)
        bit *= 2
    return flipped


def expert_part(
    weights,
    send_ref,
    gate_ref,
    up_ref,
    down_ref,
    rows,
    part,
    pairs,
    mid,
    cross,
    done,
    back,
    far_send,
    far_recv,
    near_send,
    near_recv,
    sum_send,
    sum_recv,
    back_send,
    back_recv,
):
    shards, ranks = lax.axis_size("sp"), lax.axis_size("tp")
    me, rank = lax.axis_index("sp"), lax.axis_index("tp")
    cap = send_ref.shape[0] // shards
    side, core = rank // 2, lax.rem(rank, 2)
    partner, across = rank + 1 - 2 * core, lax.rem(rank + 2, ranks)
    my_place, far_place = core * 2 + side, core * 2 + 1 - side
    block = ranks * cap

    def at(ref, index, count=1):
        return ref.at[pl.ds(pl.multiple_of(index * cap, cap), count * cap), :]

    def copy_to(source, place, send, recv, device):
        return pltpu.make_async_remote_copy(
            src_ref=source,
            dst_ref=place,
            send_sem=send,
            recv_sem=recv,
            device_id=device,
            device_id_type=pl.DeviceIdType.MESH,
        )

    def far(hop):
        target = flip(me, hop_bits(hop), shards)
        return copy_to(
            at(send_ref, target),
            at(rows, hop * ranks + my_place),
            far_send.at[hop],
            far_recv.at[hop],
            {"sp": target},
        )

    def near(kind, hop):
        place = far_place if kind == 2 else my_place
        piece = at(rows, hop * ranks + place)
        device = {"tp": across if kind == 1 else partner}
        return copy_to(piece, piece, near_send.at[kind, hop], near_recv.at[kind, hop], device)

    def pair_sum(hop):
        return copy_to(
            at(part, hop * ranks + (1 - core) * 2, 2),
            at(pairs, hop * 2, 2),
            sum_send.at[0, hop],
            sum_recv.at[0, hop],
            {"tp": partner},
        )

    def cross_sum(hop):
        return copy_to(
            at(mid, hop), at(cross, hop), sum_send.at[1, hop], sum_recv.at[1, hop], {"tp": across}
        )

    def give_back(hop):
        return copy_to(
            at(done, hop),
            at(back, me),
            back_send.at[hop],
            back_recv.at[hop],
            {"sp": flip(me, hop_bits(hop), shards)},
        )

    @pl.loop(1, shards)
    def _(hop):
        far(hop).start()

    own_rows = pltpu.make_async_copy(at(send_ref, me), at(rows, my_place), far_recv.at[0])
    own_rows.start()
    own_rows.wait()

    def share(hop):
        @pl.when(hop > 0)
        def _():
            far(hop).wait_recv()

        near(0, hop).start()
        near(1, hop).start()

    def relay(hop):
        near(1, hop).wait_recv()
        near(2, hop).start()

    def compute(hop):
        @pl.when(hop == 0)
        def _():
            for copy in weights:
                copy.wait()

        near(0, hop).wait_recv()
        near(2, hop).wait_recv()
        span = pl.ds(pl.multiple_of(hop * block, block), block)
        taken = rows[span, :]
        gate = jnp.dot(taken, gate_ref[...], preferred_element_type=jnp.float32)
        up = jnp.dot(taken, up_ref[...], preferred_element_type=jnp.float32)
        inner = (jax.nn.silu(gate) * up).astype(jnp.bfloat16)
        part[span, :] = jnp.dot(inner, down_ref[...], preferred_element_type=jnp.float32).astype(
            jnp.bfloat16
        )
        pair_sum(hop).start()

    def both(hop, place):
        mine = at(part, hop * ranks + core * 2 + place)[...].astype(jnp.float32)
        return mine + at(pairs, hop * 2 + place)[...].astype(jnp.float32)

    def add_pair(hop):
        pair_sum(hop).wait_recv()
        at(mid, hop)[...] = both(hop, 1 - side).astype(jnp.bfloat16)
        cross_sum(hop).start()

    def finish(hop):
        cross_sum(hop).wait_recv()
        total = both(hop, side) + at(cross, hop)[...].astype(jnp.float32)
        at(done, hop)[...] = total.astype(jnp.bfloat16)

        @pl.when(hop > 0)
        def _():
            give_back(hop).start()

    stages = ((share, 0), (relay, 2), (compute, 3), (add_pair, 4), (finish, 6))

    @pl.loop(0, shards + stages[-1][1])
    def _(step):
        for stage, late in stages:
            hop = step - late

            @pl.when((hop >= 0) & (hop < shards))
            def _():
                stage(hop)

    own_back = pltpu.make_async_copy(at(done, 0), at(back, me), back_recv.at[0])
    own_back.start()
    own_back.wait()

    @pl.loop(0, shards)
    def _(hop):
        for kind in range(3):
            near(kind, hop).wait_send()
        pair_sum(hop).wait_send()
        cross_sum(hop).wait_send()

        @pl.when(hop > 0)
        def _():
            far(hop).wait_send()
            give_back(hop).wait_send()
            give_back(hop).wait_recv()


def norm_rows(values):
    center = jnp.mean(values, -1, keepdims=True)
    spread = jnp.mean(jnp.square(values - center), -1, keepdims=True)
    return (values - center) * lax.rsqrt(spread + 1e-05)


def layer_kernel(
    narrow_sub_ref,
    wide_sub_ref,
    gain_ref,
    residual_ref,
    norm1_ref,
    ids_ref,
    choice_ref,
    query_narrow_ref,
    key_narrow_ref,
    value_narrow_ref,
    query_wide_ref,
    key_wide_ref,
    value_wide_ref,
    narrow_from,
    wide_from,
    gate_from,
    up_from,
    down_from,
    out_ref,
    mix_weight,
    gate_ref,
    up_ref,
    down_ref,
    hidden,
    send_ref,
    table,
    combine,
    ids_wide,
    choice_wide,
    mix_sem,
    weight_sem,
    *scratch,
):
    attend_scratch, expert_scratch = scratch[:11], scratch[11:]
    landed = attend_scratch[4]
    back = expert_scratch[6]
    top_count, rows = ids_ref.shape
    columns = table.shape[1]
    experts = lax.axis_size("sp")
    total = send_ref.shape[0]
    capacity = total // experts
    depth = narrow_from.shape[0]

    def fetch(source, place, sem):
        copy = pltpu.make_async_copy(source, place, sem)
        copy.start()
        return copy

    mixers = [
        fetch(narrow_from, mix_weight.at[pl.ds(0, depth), :], mix_sem.at[0]),
        fetch(wide_from, mix_weight.at[pl.ds(depth, depth), :], mix_sem.at[1]),
    ]
    weights = [
        fetch(gate_from, gate_ref, weight_sem.at[0]),
        fetch(up_from, up_ref, weight_sem.at[1]),
        fetch(down_from, down_ref, weight_sem.at[2]),
    ]

    def route():
        ids_wide[...] = jnp.full(ids_wide.shape, -1, jnp.int32)
        ids_wide[:, pl.ds(0, rows)] = ids_ref[...]
        choice_wide[...] = jnp.zeros_like(choice_wide)
        choice_wide[:, pl.ds(0, rows)] = choice_ref[...]
        ids = [ids_wide[pl.ds(choice, 1), :] for choice in range(top_count)]
        expert = lax.broadcasted_iota(jnp.int32, (experts, columns), 0)
        named = [(index == expert).astype(jnp.float32) for index in ids]
        later = lax.broadcasted_iota(jnp.int32, (columns, columns), 0) < lax.broadcasted_iota(
            jnp.int32, (columns, columns), 1
        )
        before = jnp.dot(
            sum(named).astype(jnp.bfloat16),
            later.astype(jnp.float32).astype(jnp.bfloat16),
            preferred_element_type=jnp.float32,
        )
        line = lax.broadcasted_iota(jnp.int32, (total, columns), 0)
        picks = jnp.zeros((total, columns), jnp.float32)
        mixing = jnp.zeros((total, columns), jnp.float32)
        for choice in range(top_count):
            held = jnp.sum(before * named[choice], 0, keepdims=True).astype(jnp.int32)
            taken = (ids[choice] * capacity + held == line) & (ids[choice] >= 0)
            picks = jnp.where(taken, 1.0, picks)
            mixing = jnp.where(taken, choice_wide[pl.ds(choice, 1), :], mixing)
        table[...] = picks.astype(jnp.bfloat16)
        combine[...] = mixing.T
        hidden[...] = jnp.zeros_like(hidden)

    drain = attend_part(
        route,
        narrow_sub_ref,
        wide_sub_ref,
        gain_ref,
        query_narrow_ref,
        key_narrow_ref,
        value_narrow_ref,
        query_wide_ref,
        key_wide_ref,
        value_wide_ref,
        *attend_scratch,
    )
    for copy in mixers:
        copy.wait()
    mix = jnp.dot(landed[...], mix_weight[...], preferred_element_type=jnp.float32)
    held = residual_scale * residual_ref[...].astype(jnp.float32) + mix
    hidden[pl.ds(0, rows), :] = (norm_rows(held) * norm1_ref[...]).astype(jnp.bfloat16)
    send_ref[...] = jnp.dot(
        table[...], hidden[...], preferred_element_type=jnp.float32
    ).astype(jnp.bfloat16)
    expert_part(weights, send_ref, gate_ref, up_ref, down_ref, *expert_scratch)
    coarse = combine[...].astype(jnp.bfloat16)
    fine = (combine[...] - coarse.astype(jnp.float32)).astype(jnp.bfloat16)
    routed = jnp.dot(coarse, back[...], preferred_element_type=jnp.float32) + jnp.dot(
        fine, back[...], preferred_element_type=jnp.float32
    )
    tokens = residual_scale * hidden[pl.ds(0, rows), :].astype(jnp.float32) + routed[:rows]
    out_ref[...] = norm_rows(tokens)
    drain()


def whole_layer(
    residual,
    attend_args,
    subtract_narrow,
    subtract_wide,
    head_gain,
    out_weights,
    norm1_gain,
    norm2_gain,
    expert_ids,
    expert_weight,
    expert_weights,
    capacity,
):
    shards, ranks = lax.axis_size("sp"), lax.axis_size("tp")
    head_count, lanes = subtract_narrow.shape[0], head_gain.shape[0]
    tok_rows = attend_args[0].shape[0]
    rows, width = residual.shape
    tokens, layers = shards * tok_rows, 2 * head_count
    heads = layers * ranks
    total = shards * capacity
    vmem = pl.BlockSpec(memory_space=pltpu.VMEM)
    smem = pl.BlockSpec(memory_space=pltpu.SMEM)
    dma = pltpu.SemaphoreType.DMA

    def buffer(*shape):
        return pltpu.VMEM(shape, jnp.bfloat16)

    columns = -(-rows // 128) * 128
    normed = pl.pallas_call(
        layer_kernel,
        out_shape=jax.ShapeDtypeStruct((rows, width), jnp.float32),
        in_specs=[smem, smem] + [vmem] * 5 + [pl.BlockSpec(memory_space=pl.ANY)] * 11,
        out_specs=vmem,
        scratch_shapes=[buffer(heads * lanes, width)]
        + [buffer(*part.shape) for part in expert_weights]
        + [
            buffer(columns, width),
            buffer(total, width),
            buffer(total, columns),
            pltpu.VMEM((columns, total), jnp.float32),
            pltpu.VMEM(expert_ids.shape[1:] + (columns,), jnp.int32),
            pltpu.VMEM(expert_ids.shape[1:] + (columns,), jnp.float32),
            dma((2,)),
            dma((3,)),
            buffer(2, layers * tok_rows, lanes),
            buffer(2, tokens, lanes),
            buffer(tokens, 2 * lanes),
            buffer(layers * tok_rows, lanes),
            buffer(rows, heads * lanes),
            dma((5, layers)),
            dma((5, layers)),
            dma((3, layers)),
            dma((3, layers)),
            dma((layers, ranks)),
            dma((heads,)),
        ]
        + [buffer(count * total, width) for count in (ranks, ranks, 2, 1, 1, 1, 1)]
        + [
            dma((shards,)),
            dma((shards,)),
            dma((3, shards)),
            dma((3, shards)),
            dma((2, shards)),
            dma((2, shards)),
            dma((shards,)),
            dma((shards,)),
        ],
        compiler_params=pltpu.CompilerParams(
            collective_id=0, has_side_effects=True, vmem_limit_bytes=62 * 1024 * 1024
        ),
    )(
        subtract_narrow,
        subtract_wide,
        head_gain[None],
        residual,
        norm1_gain[None],
        expert_ids.T,
        expert_weight.T,
        *attend_args,
        *out_weights,
        *expert_weights,
    )
    return (normed * norm2_gain).astype(jnp.bfloat16)


def on_device(
    residual,
    query_narrow,
    key_narrow,
    value_narrow,
    query_wide,
    key_wide,
    value_wide,
    subtract_narrow,
    subtract_wide,
    head_gain,
    out_narrow,
    out_wide,
    norm1_gain,
    norm2_gain,
    expert_ids,
    expert_weight,
    gate_proj,
    up_proj,
    down_proj,
):
    tok_rows = query_narrow.shape[0]
    head_count = subtract_narrow.shape[0]
    value_size = head_gain.shape[0]
    local_rows, top_count = expert_ids.shape
    experts = lax.axis_size("sp")
    capacity = max(2, 3 * local_rows * top_count // (2 * experts))
    padded = -(-capacity // 16) * 16
    if (
        head_split_fits(
            tok_rows,
            local_rows,
            lax.axis_size("tp"),
            head_count,
            experts,
            value_size,
            tuple(part.shape[1] // (2 * head_count) for part in (key_narrow, key_wide)),
        )
        and lax.axis_size("tp") == 4
        and top_count == 2
        and experts & (experts - 1) == 0
        and 4 * experts * padded * residual.shape[1] < 2**23
    ):
        return whole_layer(
            residual,
            (query_narrow, key_narrow, value_narrow, query_wide, key_wide, value_wide),
            subtract_narrow,
            subtract_wide,
            head_gain,
            (out_narrow, out_wide),
            norm1_gain,
            norm2_gain,
            expert_ids,
            expert_weight,
            (gate_proj[0], up_proj[0], down_proj[0]),
            padded,
        )
    narrow_queries = query_narrow.reshape(tok_rows, head_count, 2, -1)
    wide_queries = query_wide.reshape(tok_rows, head_count, 2, -1)
    narrow_start = start_carry(head_count, tok_rows, value_size)
    wide_start = start_carry(head_count, tok_rows, value_size)
    narrow_state = absorb_keys(
        narrow_start,
        narrow_queries,
        lax.all_gather(key_narrow, "sp", axis=0, tiled=True),
        lax.all_gather(value_narrow, "sp", axis=0, tiled=True),
        tok_rows,
    )
    wide_state = absorb_keys(
        wide_start,
        wide_queries,
        lax.all_gather(key_wide, "sp", axis=0, tiled=True),
        lax.all_gather(value_wide, "sp", axis=0, tiled=True),
        tok_rows,
    )
    attended_narrow = finish_heads(narrow_state, subtract_narrow, head_gain)
    attended_wide = finish_heads(wide_state, subtract_wide, head_gain)
    full_narrow, full_wide = (
        lax.all_to_all(attended_narrow, "tp", split_axis=0, concat_axis=1, tiled=True),
        lax.all_to_all(attended_wide, "tp", split_axis=0, concat_axis=1, tiled=True),
    )
    mix = jnp.dot(full_narrow, out_narrow, preferred_element_type=jnp.float32) + jnp.dot(
        full_wide, out_wide, preferred_element_type=jnp.float32
    )
    hidden = layer_norm(residual_scale * residual.astype(jnp.float32) + mix, norm1_gain).astype(
        jnp.bfloat16
    )
    flat_ids = expert_ids.reshape(-1)
    onehot = (flat_ids[:, None] == jnp.arange(experts, dtype=jnp.int32)[None, :]).astype(jnp.int32)
    before = jnp.cumsum(onehot, 0) - onehot
    position = jnp.sum(before * onehot, 1)
    slots = (flat_ids * capacity + position).reshape(local_rows, top_count)
    dispatch_table = jnp.any(
        jnp.arange(experts * capacity, dtype=jnp.int32)[:, None, None] == slots[None], -1
    ).astype(jnp.bfloat16)
    outgoing = jnp.dot(dispatch_table, hidden, preferred_element_type=jnp.float32).astype(
        jnp.bfloat16
    )
    outgoing = outgoing.reshape(experts, capacity, -1)
    gathered = lax.all_gather(
        lax.all_to_all(outgoing, "sp", split_axis=0, concat_axis=0, tiled=True),
        "tp",
        axis=1,
        tiled=True,
    )
    flat_rows = gathered.reshape(-1, gathered.shape[2])
    gate_part = jnp.dot(flat_rows, gate_proj[0], preferred_element_type=jnp.float32)
    up_part = jnp.dot(flat_rows, up_proj[0], preferred_element_type=jnp.float32)
    inner = (jax.nn.silu(gate_part) * up_part).astype(jnp.bfloat16)
    partial_out = jnp.dot(inner, down_proj[0], preferred_element_type=jnp.float32).reshape(
        gathered.shape
    )
    summed = lax.psum_scatter(
        partial_out.astype(jnp.bfloat16), "tp", scatter_dimension=1, tiled=True
    )
    returned = lax.all_to_all(summed, "sp", split_axis=0, concat_axis=0, tiled=True)
    returned_flat = returned.reshape(experts * capacity, -1)
    picked = returned_flat[slots].astype(jnp.float32)
    routed = jnp.sum(expert_weight[..., None] * picked, 1)
    return layer_norm(residual_scale * hidden.astype(jnp.float32) + routed, norm2_gain).astype(
        jnp.bfloat16
    )


def solution(mesh):
    placed = (
        P(("sp", "tp"), None),
        P("sp", "tp"),
        P("sp", "tp"),
        P("sp", "tp"),
        P("sp", "tp"),
        P("sp", "tp"),
        P("sp", "tp"),
        P("tp"),
        P("tp"),
        P(),
        P(),
        P(),
        P(),
        P(),
        P(("sp", "tp"), None),
        P(("sp", "tp"), None),
        P("sp", None, "tp"),
        P("sp", None, "tp"),
        P("sp", "tp", None),
    )
    return jax.shard_map(
        on_device, mesh=mesh, in_specs=placed, out_specs=P(("sp", "tp"), None), check_vma=False
    )
```
